256 devices in a mesh: sp: 32 (over z, y), fs: 4 (over x), tp: 2 (over core).
Axes of the slice: x: 4, y: 4, z: 8, core: 2. Of those that a mesh axis runs over, the one named last changes fastest.
Arguments:
- tokens: bfloat16 [4, 4096, 4096], P('fs', 'sp'), may hold values from -6 to 6
- norm_gain: float32 [4096], replicated, may hold values from 0.1 to 1.9
- pool_proj: bfloat16 [4096, 1024], P(('sp', 'fs'), 'tp'), may hold values from -0.09375 to 0.09375
- query_proj: bfloat16 [4096, 1024], P(('sp', 'fs'), 'tp'), may hold values from -0.09375 to 0.09375
- key_proj: bfloat16 [4096, 1024], P(('sp', 'fs'), 'tp'), may hold values from -0.09375 to 0.09375
- value_proj: bfloat16 [4096, 1024], P(('sp', 'fs'), 'tp'), may hold values from -0.09375 to 0.09375
- pool_map: bfloat16 [4, 256, 256], replicated, may hold values from -0.375 to 0.375
- pool_scale: float32 [1024], replicated, may hold values from 0.1 to 1.9
- decay_rate: float32 [4], P('tp'), may hold values from 2e-05 to 0.034
- start_state: float32 [4, 4, 256, 256], P('fs', 'tp', 'sp'), may hold values from -96 to 96
- pool_back: bfloat16 [1024, 4096], P('tp', ('sp', 'fs')), may hold values from -0.125 to 0.125
- retention_back: bfloat16 [1024, 4096], P('tp', ('sp', 'fs')), may hold values from -0.125 to 0.125
Outputs:
- mixed: bfloat16 [4, 4096, 4096], P('fs', ('sp', 'tp'))
The draws below stay inside these ranges and needn't reach their ends.
All inputs are finite; a program needn't handle non-finite values.
Results may differ from the reference program's by a relative error of at most 0.014.
Values may be sent and summed in bfloat16 or wider, within the bound.
No kernel may reach another device: no remote copies, remote signals or barrier semaphores. Data moves between devices by JAX's collectives and lax.ppermute only.
A program may use at most 128 MiB of HBM per device.

```python
import jax
import jax.numpy as jnp
from jax import lax

DMODEL = 4096
GROUPS = 4
GROUP_DIM = 256
RET_HEADS = 4
HEAD_DIM = 256
BLOCK = 128
HALO = 16
POOL_WIDTH = 1024
RET_WIDTH = 1024
SEQS = 4
SEQ_LEN = 4096


def draw_decay_rate(key, part):
    order_key, level_key = jax.random.split(jax.random.fold_in(key, 7))
    order = jax.random.permutation(order_key, RET_HEADS)
    quick = order < RET_HEADS // 2
    level = jax.random.uniform(level_key, (RET_HEADS,), jnp.float32)
    quick_rate = jnp.exp(jnp.log(0.01) + level * (jnp.log(1.0 / 30.0) - jnp.log(0.01)))
    slow_rate = jnp.exp(jnp.log(2e-05) + level * (jnp.log(0.00012) - jnp.log(2e-05)))
    return jnp.where(quick, quick_rate, slow_rate).astype(jnp.float32)


def levels(rng, dims, cuts, smallest, high):
    factor_of = 1.0
    for dim, parts in cuts:
        steps = jax.random.uniform(jax.random.fold_in(jax.random.fold_in(rng, 6), dim), (parts,), jnp.float32, smallest / len(cuts), high / len(cuts))
        factor_of = factor_of * jnp.repeat(jnp.exp(steps), dims[dim] // parts).reshape((-1,) + (1,) * (len(dims) - 1 - dim))
    return factor_of


def normal_values(stream_key, dims, spread, most, cuts=(), held_as=jnp.bfloat16):
    drawn = jax.random.normal(stream_key, dims, jnp.float32) * spread
    if len(cuts) > 0:
        drawn = levels(stream_key, dims, cuts, -0.22, 0.18) * drawn
    return jnp.clip(drawn, min=-most, max=most).astype(held_as)


def setup_inputs(seed: int = 0) -> dict:
    streams_of = jax.random.split(jax.random.key(seed), 13)
    tokens = normal_values(streams_of[0], (SEQS, SEQ_LEN, DMODEL), 1.0, 6.0, ((0, 4), (1, 32)))
    norm_gain = jnp.clip(1.0 + 0.18 * jax.random.normal(streams_of[1], (DMODEL,), jnp.float32), 0.1, 1.9)
    pool_proj = normal_values(streams_of[2], (DMODEL, POOL_WIDTH), DMODEL ** -0.5, 0.09375, ((0, 128), (1, 2)))
    query_proj = normal_values(streams_of[3], (DMODEL, RET_WIDTH), DMODEL ** -0.5, 0.09375, ((0, 128), (1, 2)))
    key_proj = normal_values(streams_of[4], (DMODEL, RET_WIDTH), DMODEL ** -0.5, 0.09375, ((0, 128), (1, 2)))
    value_proj = normal_values(streams_of[5], (DMODEL, RET_WIDTH), DMODEL ** -0.5, 0.09375, ((0, 128), (1, 2)))
    pool_map = normal_values(streams_of[6], (GROUPS, GROUP_DIM, GROUP_DIM), GROUP_DIM ** -0.5, 0.375)
    pool_scale = jnp.clip(1.0 + 0.18 * jax.random.normal(streams_of[7], (POOL_WIDTH,), jnp.float32), 0.1, 1.9)
    decay_rate = draw_decay_rate(jax.random.fold_in(streams_of[12], 71), 0)
    start_state = normal_values(streams_of[9], (SEQS, RET_HEADS, HEAD_DIM, HEAD_DIM), 16.0, 96.0, ((0, 4), (1, 2), (2, 32)), jnp.float32)
    pool_back = normal_values(streams_of[10], (POOL_WIDTH, DMODEL), (POOL_WIDTH + RET_WIDTH) ** -0.5, 0.125, ((0, 2), (1, 128)))
    retention_back = normal_values(streams_of[11], (RET_WIDTH, DMODEL), (POOL_WIDTH + RET_WIDTH) ** -0.5, 0.125, ((0, 2), (1, 128)))
    return {"tokens": tokens, "norm_gain": norm_gain, "pool_proj": pool_proj, "query_proj": query_proj, "key_proj": key_proj, "value_proj": value_proj, "pool_map": pool_map, "pool_scale": pool_scale, "decay_rate": decay_rate, "start_state": start_state, "pool_back": pool_back, "retention_back": retention_back}


eps = 1e-06
rope_base = 10000.0
highest_precision = lax.Precision.HIGHEST
window_list = (2, 4, 8, 16)

def rotate(values, positions):
    half_dim = values.shape[-1] // 2
    inv_freq = 1.0 / rope_base ** jnp.linspace(0.0, 1.0, half_dim, dtype=jnp.float32)
    angles = positions.astype(jnp.float32)[:, None] * inv_freq[None, :]
    cosine = jnp.cos(angles)[:, None, :]
    sine = jnp.sin(angles)[:, None, :]
    first_half = values[..., :half_dim]
    second_half = values[..., half_dim:]
    return jnp.concatenate([first_half * cosine - second_half * sine, first_half * sine + second_half * cosine], axis=-1)

def trailing_sums(extended, length):
    begin = extended.shape[0] - length
    running = extended[begin:]
    results = []
    for behind in range(1, 16):
        running = running + extended[begin - behind:begin - behind + length]
        if behind + 1 in window_list:
            results.append(running)
    return results

def reshape_blocks(array):
    return array.reshape((array.shape[0] // BLOCK, BLOCK) + array.shape[1:])

def block_retention(queries, keys_in, values_in, decay_rate, initial):
    length, head_count, head_dim = queries.shape
    within = jnp.arange(BLOCK, dtype=jnp.float32)
    distance = within[:, None] - within[None, :]
    decay_mask = jnp.where(distance[None] >= 0, jnp.exp(-jnp.maximum(distance, 0.0)[None] * decay_rate[:, None, None]), 0.0)
    query_decay_factor = jnp.exp(-(within + 1.0)[:, None] * decay_rate[None, :])
    key_decay_factor = jnp.exp(-(BLOCK - 1.0 - within)[:, None] * decay_rate[None, :])
    block_decay_factor = jnp.exp(-BLOCK * decay_rate)

    def advance(state_carry, inputs):
        block_queries, block_keys, block_values = inputs
        scores = jnp.einsum('ihk,jhk->hij', block_queries, block_keys, precision=highest_precision) * decay_mask
        inside = jnp.einsum('hij,jhv->ihv', scores, block_values, precision=highest_precision)
        across_blocks = jnp.einsum('bzy,zyx->bzx', block_queries * query_decay_factor[:, :, None], state_carry, precision=highest_precision)
        state_carry = state_carry * block_decay_factor[:, None, None] + jnp.einsum('flm,fld->lmd', block_keys * key_decay_factor[:, :, None], block_values, precision=highest_precision)
        return (state_carry, inside + across_blocks)
    final_state, outputs = lax.scan(advance, initial, (reshape_blocks(queries), reshape_blocks(keys_in), reshape_blocks(values_in)))
    return (outputs.reshape(length, head_count, values_in.shape[-1]), final_state)

def reference(tokens, norm_gain, pool_proj, query_proj, key_proj, value_proj, pool_map, pool_scale, decay_rate, start_state, pool_back, retention_back):
    weights_back = jnp.concatenate([pool_back, retention_back], axis=0)

    def one_sequence(operands):
        sequence, initial = operands
        floats = sequence.astype(jnp.float32)
        normed = (floats * lax.rsqrt(lax.optimization_barrier(jnp.mean(floats * floats, axis=-1, keepdims=True)) + eps) * norm_gain).astype(jnp.bfloat16)
        pool_in = jnp.dot(normed, pool_proj, preferred_element_type=jnp.float32).astype(jnp.bfloat16)
        query_bf = jnp.dot(normed, query_proj, preferred_element_type=jnp.float32).astype(jnp.bfloat16)
        key_bf = jnp.dot(normed, key_proj, preferred_element_type=jnp.float32).astype(jnp.bfloat16)
        value_bf = jnp.dot(normed, value_proj, preferred_element_type=jnp.float32).astype(jnp.bfloat16)
        positions = jnp.arange(SEQ_LEN, dtype=jnp.int32)
        extended = jnp.concatenate([jnp.zeros((HALO, POOL_WIDTH), jnp.float32), pool_in.astype(jnp.float32)], axis=0)
        sums_all = trailing_sums(extended, SEQ_LEN)
        pieces = []
        for group_idx in range(GROUPS):
            lower = group_idx * GROUP_DIM
            chosen = sums_all[group_idx][:, lower:lower + GROUP_DIM]
            counts = jnp.minimum(window_list[group_idx], positions + 1).astype(jnp.float32)
            inputs = extended[HALO:, lower:lower + GROUP_DIM]
            differ = (chosen / counts[:, None] - inputs).astype(jnp.bfloat16)
            pieces.append(jnp.dot(differ, pool_map[group_idx], preferred_element_type=jnp.float32))
        pool_out = (jnp.concatenate(pieces, axis=1) * pool_scale).astype(jnp.bfloat16)
        queries = rotate(query_bf.astype(jnp.float32).reshape(SEQ_LEN, RET_HEADS, HEAD_DIM), positions)
        keys_in = rotate(key_bf.astype(jnp.float32).reshape(SEQ_LEN, RET_HEADS, HEAD_DIM), positions) * HEAD_DIM ** (-0.5)
        values_in = value_bf.astype(jnp.float32).reshape(SEQ_LEN, RET_HEADS, HEAD_DIM)
        retained_output, final_state = block_retention(queries, keys_in, values_in, decay_rate, initial)
        retained_output = retained_output * lax.rsqrt(lax.optimization_barrier(jnp.mean(retained_output * retained_output, axis=-1, keepdims=True)) + eps)
        ret_out = retained_output.reshape(SEQ_LEN, RET_WIDTH).astype(jnp.bfloat16)
        joined = jnp.concatenate([pool_out, ret_out], axis=1)
        return jnp.dot(joined, weights_back, preferred_element_type=jnp.float32).astype(jnp.bfloat16)
    return lax.map(one_sequence, (tokens, start_state))
```

```python
import jax
import jax.numpy as jnp
from jax import lax
from jax.experimental import pallas as pl
from jax.experimental.pallas import tpu as pltpu
from jax.sharding import Mesh
from jax.sharding import PartitionSpec as P

NZ, NY, NX = 8, 4, 4
SPAN = 512
HALO = 16
HEAD = 256
HALF = 128
eps = 1e-06
rope_base = 10000.0

bf16 = jnp.bfloat16
f32 = jnp.float32


def ring(n, k):
    return [(i, (i + k) % n) for i in range(n)]


def line(n, k):
    return [(i, i + k) for i in range(n - k)]


def to_heads(k):
    return [(2 * y + c, 2 * (2 * c + (k + y) % 2) + y // 2) for y in range(NY) for c in range(2)]


SWAP = [(0, 1), (1, 0)]


def swap(a):
    return lax.ppermute(a, "c", SWAP)


def direct(a, axis, n):
    return [a] + [lax.ppermute(a, axis, ring(n, k)) for k in range(1, n)]


def z_ring(a):
    chunks = [None] * NZ
    chunks[0] = a
    up = down = a
    for s in range(1, 4):
        up = lax.ppermute(up, "z", ring(NZ, 1))
        down = lax.ppermute(down, "z", ring(NZ, -1))
        chunks[NZ - s], chunks[s] = up, down
    return chunks


def by_head(parts, y):
    even = y % 2 == 0
    first = jnp.where(even, parts[0], parts[1])
    second = jnp.where(even, parts[1], parts[0])
    r0 = lax.ppermute(first, ("y", "c"), to_heads(0))
    r1 = lax.ppermute(second, ("y", "c"), to_heads(1))
    return jnp.where(even, r0, r1), jnp.where(even, r1, r0)


def project_body(at, *refs):
    toks = refs[0:4]
    a_refs = refs[4:13]
    b_refs = refs[13:17]
    out, lhs, rhs = refs[17:20]
    z, y = at[0], at[1]
    for k in range(NY):
        rows = pl.ds(pl.multiple_of(((y + NY - k) % NY) * HALF, HALF), HALF)
        for kz in range(NZ):
            lhs[rows, kz * 256:(kz + 1) * 256] = toks[k][(z + kz) % NZ]
    i = 0
    for kz in range(NZ):
        if kz == 4:
            rhs[1024:1152, :512] = a_refs[7][...]
            rhs[1152:1280, :512] = a_refs[8][...]
        else:
            rhs[kz * 256:(kz + 1) * 256, :512] = a_refs[i][...]
            i += 1
        for kx in range(NX):
            rhs[kz * 256 + kx * 64:kz * 256 + (kx + 1) * 64, 512:] = b_refs[kx][kz * 64:(kz + 1) * 64, :]
    out[...] = jnp.dot(lhs[...], rhs[...], preferred_element_type=f32)


def project(at, toks, a_chunks, b_chunks):
    vm = pl.BlockSpec(memory_space=pltpu.VMEM)
    return pl.pallas_call(
        project_body,
        in_specs=[pl.BlockSpec(memory_space=pltpu.SMEM)] + [vm] * 17,
        out_specs=vm,
        out_shape=jax.ShapeDtypeStruct((SPAN, 1024), f32),
        scratch_shapes=[pltpu.VMEM((SPAN, 2048), bf16), pltpu.VMEM((2048, 1024), bf16)],
        name="project",
    )(at, *toks, *a_chunks, *b_chunks)


def back_body(at, act, w0, w1, w2, w3, o0, o1, o2, o3, rhs):
    z, y, x = at[0], at[1], at[2]
    for kx, w in enumerate((w0, w1, w2, w3)):
        for kz in range(NZ):
            rhs[(z + kz) % NZ, :, (x + NX - kx) % NX] = w[kz]
    wt = rhs[...].reshape(2048, SPAN)
    for k, o in enumerate((o0, o1, o2, o3)):
        rows = act[pl.ds(pl.multiple_of(((y + k) % NY) * HALF, HALF), HALF), :]
        r = lax.dot_general(rows, wt, (((1,), (1,)), ((), ())), preferred_element_type=f32)
        o[...] = r.astype(bf16)


def back(at, act, ws):
    vm = pl.BlockSpec(memory_space=pltpu.VMEM)
    return pl.pallas_call(
        back_body,
        in_specs=[pl.BlockSpec(memory_space=pltpu.SMEM)] + [vm] * 5,
        out_specs=[vm] * 4,
        out_shape=[jax.ShapeDtypeStruct((HALF, 2048), bf16)] * 4,
        scratch_shapes=[pltpu.VMEM((NZ, 2, NX, 32, SPAN), bf16)],
        name="back",
    )(at, act, *ws)


def on_device(tokens, norm_gain, pool_proj, query_proj, key_proj, value_proj, pool_map, pool_scale,
              decay_rate, start_state, pool_back, retention_back):
    z, y, x, c = (lax.axis_index(a) for a in ("z", "y", "x", "c"))
    at = jnp.stack([z, y, x, c]).astype(jnp.int32)

    parts = []
    for p in range(2):
        cols = slice(p * HEAD, (p + 1) * HEAD)
        w = jnp.concatenate([m[:, cols] for m in (pool_proj, query_proj, key_proj, value_proj)], axis=1)
        s = start_state[0, p]
        hi = s.astype(bf16)
        lo = (s - hi.astype(f32)).astype(bf16)
        pad = jnp.concatenate([hi, lo, jnp.zeros((8, 512), bf16)], axis=1)
        parts.append(jnp.concatenate([w, pad], axis=0))
    w_even, w_odd = by_head(parts, y)
    shard_a = jnp.concatenate([w_even[:32, :512], w_odd[:32, :512]], axis=0)
    shard_b = jnp.concatenate([w_even[:32, 512:], w_odd[:32, 512:], w_even[32:, :512], w_odd[32:, :512]], axis=0)

    floats = tokens[0].astype(f32)
    normed = (floats * lax.rsqrt(jnp.mean(floats * floats, axis=-1, keepdims=True) + eps) * norm_gain).astype(bf16)
    mine = lax.dynamic_index_in_dim(normed.reshape(HALF, NZ, 2, 256), c, 2, keepdims=False)
    lane_in = lax.broadcasted_iota(jnp.int32, (256, 256), 0)
    lane_out = lax.broadcasted_iota(jnp.int32, (256, 256), 1)
    source = (lane_out % 64) // 32 * 128 + (x + NX - lane_out // 64) % NX * 32 + lane_out % 32
    order = (lane_in == source).astype(bf16)
    toks = jnp.einsum("tzk,kl->ztl", mine, order, preferred_element_type=f32).astype(bf16)
    toks = direct(toks, "y", NY)

    plane_a = jnp.concatenate(direct(shard_a, "x", NX), axis=0)
    a_chunks = z_ring(plane_a)
    half_up = lax.ppermute(a_chunks[5][:128], "z", ring(NZ, 1))
    half_down = lax.ppermute(a_chunks[3][128:], "z", ring(NZ, -1))
    a_list = a_chunks[:4] + a_chunks[5:] + [half_up, half_down]
    b_z = z_ring(shard_b)
    b_z[4] = lax.ppermute(b_z[5], "z", ring(NZ, 1))
    plane_b = jnp.concatenate([b[:64] for b in b_z], axis=0)
    b_list = direct(plane_b, "x", NX)

    parts = []
    for p in range(2):
        rows = slice(p * HEAD, (p + 1) * HEAD)
        parts.append(jnp.concatenate([pool_back[rows].T, retention_back[rows].T], axis=1))
    o_even, o_odd = by_head(parts, y)
    shard_o = jnp.concatenate([o_even, o_odd], axis=0)
    o_z = z_ring(shard_o)
    o_z[4] = lax.ppermute(o_z[5], "z", ring(NZ, 1))
    plane_o = jnp.stack(o_z).reshape(NZ, 2, 32, SPAN)
    o_list = direct(plane_o, "x", NX)

    st = jnp.stack([b[64:] for b in b_z])
    st = (st[..., :256].astype(f32) + st[..., 256:].astype(f32)).reshape(NZ, 2, 8, 2, HALF)
    keep = lax.dynamic_index_in_dim(st, c, 3, keepdims=False)
    give = lax.dynamic_index_in_dim(st, 1 - c, 3, keepdims=False)
    got = swap(give)
    both = jnp.where(c == 0, jnp.stack([keep, got], 1), jnp.stack([got, keep], 1))
    start = jnp.roll(both.reshape(NZ, 32, HALF), z, axis=0).reshape(HEAD, HALF)

    rates = jnp.where(c == y // 2, decay_rate, swap(decay_rate))
    rate = jnp.where(y % 2 == 0, rates[0], rates[1])
    scale = lax.dynamic_slice_in_dim(pool_scale, y * HEAD, HEAD, 0)
    group_map = lax.dynamic_index_in_dim(pool_map, y, 0, keepdims=False)

    within = jnp.arange(SPAN, dtype=f32)
    positions = (jnp.arange(SPAN, dtype=jnp.int32) + z * SPAN)
    inv_freq = 1.0 / rope_base ** jnp.linspace(0.0, 1.0, HALF, dtype=f32)
    angles = positions.astype(f32)[:, None] * inv_freq[None, :]
    cosine, sine = jnp.cos(angles), jnp.sin(angles)
    distance = within[:, None] - within[None, :]
    mask = jnp.where(distance >= 0, jnp.exp(-jnp.maximum(distance, 0.0) * rate), 0.0)
    key_decay = jnp.exp(-(SPAN - 1.0 - within) * rate)[:, None]
    query_decay = jnp.exp(-(within + 1.0) * rate)[:, None]
    span_decay = jnp.exp(-SPAN * rate)

    own = project(at, toks, a_list, b_list)
    v_own = own[:, 768:].reshape(SPAN, 2, HALF)
    v_give = lax.dynamic_index_in_dim(v_own, 1 - c, 1, keepdims=False)
    v_keep = lax.dynamic_index_in_dim(v_own, c, 1, keepdims=False)
    got = swap(jnp.concatenate([own[:, :768], v_give], axis=1).astype(bf16)).astype(f32)
    pool_in = (own[:, :256] + got[:, :256]).astype(bf16)
    query = (own[:, 256:512] + got[:, 256:512]).astype(bf16).astype(f32)
    key = (own[:, 512:768] + got[:, 512:768]).astype(bf16).astype(f32)
    value = (v_keep + got[:, 768:]).astype(bf16)

    def rotate(v):
        a, b = v[:, :HALF], v[:, HALF:]
        return jnp.concatenate([a * cosine - b * sine, a * sine + b * cosine], axis=1)

    rk = rotate(key) * HEAD ** -0.5
    state = lax.dot_general((rk * key_decay).astype(bf16), value, (((0,), (0,)), ((), ())), preferred_element_type=f32)
    state = state + jnp.where(z == 0, span_decay, 0.0) * start
    sent = state.astype(bf16)
    r1, r2, r3 = (lax.ppermute(sent, "z", line(NZ, k)).astype(f32) for k in (1, 2, 3))
    near = r1 + span_decay * (r2 + span_decay * r3)
    far = lax.ppermute((state + span_decay * near).astype(bf16), "z", line(NZ, 4)).astype(f32)
    carried = near + span_decay * span_decay * span_decay * far + jnp.where(z == 0, 1.0, 0.0) * start

    rq = rotate(query)
    scores = lax.dot_general(rq.astype(bf16), rk.astype(bf16), (((1,), (1,)), ((), ())), preferred_element_type=f32)
    inside = jnp.dot((scores * mask).astype(bf16), value, preferred_element_type=f32)
    across = jnp.dot((rq * query_decay).astype(bf16), carried.astype(bf16), preferred_element_type=f32)
    ret = inside + across
    other = swap(ret)
    ret = jnp.where(c == 0, jnp.concatenate([ret, other], 1), jnp.concatenate([other, ret], 1))
    ret_out = (ret * lax.rsqrt(jnp.mean(ret * ret, axis=-1, keepdims=True) + eps)).astype(bf16)

    before = lax.ppermute(pool_in[SPAN - HALO:], "z", line(NZ, 1))
    ext = jnp.concatenate([before, pool_in], axis=0).astype(f32)
    sums = ext
    chosen = None
    n = SPAN + HALO
    for g in range(4):
        w = 2 ** g
        sums = sums + jnp.concatenate([jnp.zeros((w, HEAD), f32), sums[: n - w]], axis=0)
        chosen = sums if chosen is None else jnp.where(y == g, sums, chosen)
    window = lax.shift_left(jnp.int32(2), y)
    counts = jnp.minimum(window, positions + 1).astype(f32)[:, None]
    differ = (chosen[HALO:] / counts - ext[HALO:]).astype(bf16)
    pool_out = (jnp.dot(differ, group_map, preferred_element_type=f32) * scale).astype(bf16)

    act = jnp.concatenate([pool_out, ret_out], axis=1)
    shares = back(at, act, o_list)
    total = shares[0].astype(f32)
    for k in range(1, NY):
        total = total + lax.ppermute(shares[k], "y", ring(NY, k)).astype(f32)
    total = total.astype(bf16).reshape(2, 64, 2048)
    keep = lax.dynamic_index_in_dim(total, c, 0, keepdims=False).reshape(64, NZ, 256)
    got = swap(lax.dynamic_index_in_dim(total, 1 - c, 0, keepdims=False)).reshape(64, NZ, 256)
    mixed = jnp.where(c == 0, jnp.stack([keep, got], 2), jnp.stack([got, keep], 2))
    return mixed.reshape(1, 64, 4096)


def solution(mesh):
    torus = Mesh(mesh.devices.reshape(NZ, NY, NX, 2), ("z", "y", "x", "c"))
    sp, sp_fs = ("z", "y"), ("z", "y", "x")
    placed = (
        P("x", sp, None), P(), P(sp_fs, "c"), P(sp_fs, "c"), P(sp_fs, "c"), P(sp_fs, "c"), P(), P(),
        P("c"), P("x", "c", sp, None), P("c", sp_fs), P("c", sp_fs),
    )
    return jax.shard_map(on_device, mesh=torus, in_specs=placed, out_specs=P("x", ("z", "y", "c"), None), check_vma=False)
```

```python
import jax
import jax.numpy as jnp
from jax import lax
from jax.experimental import pallas as pl
from jax.experimental.pallas import tpu as pltpu
from jax.sharding import Mesh
from jax.sharding import PartitionSpec as P

NZ, NY, NX = 8, 4, 4
SPAN = 512
HALO = 16
HEAD = 256
HALF = 128
eps = 1e-06
rope_base = 10000.0

bf16 = jnp.bfloat16
f32 = jnp.float32


def ring(n, k):
    return [(i, (i + k) % n) for i in range(n)]


def line(n, k):
    return [(i, i + k) for i in range(n - k)]


def to_heads(k):
    return [(2 * y + c, 2 * (2 * c + (k + y) % 2) + y // 2) for y in range(NY) for c in range(2)]


SWAP = [(0, 1), (1, 0)]


def swap(a):
    return lax.ppermute(a, "c", SWAP)


def direct(a, axis, n):
    return [a] + [lax.ppermute(a, axis, ring(n, k)) for k in range(1, n)]


def z_ring(a):
    chunks = [None] * NZ
    chunks[0] = a
    up = down = a
    for s in range(1, 4):
        up = lax.ppermute(up, "z", ring(NZ, 1))
        down = lax.ppermute(down, "z", ring(NZ, -1))
        chunks[NZ - s], chunks[s] = up, down
    return chunks


VM = pl.BlockSpec(memory_space=pltpu.VMEM)
SM = pl.BlockSpec(memory_space=pltpu.SMEM)
ANY = pl.BlockSpec(memory_space=pl.ANY)
ROWS = 112


def pack_body(at, pool, query, key, value, state, pback, rback, s0, s1):
    y = at[1]
    eye = (lax.broadcasted_iota(jnp.int32, (32, 32), 0) == lax.broadcasted_iota(jnp.int32, (32, 32), 1)).astype(bf16)

    def turned(ref, rows):
        return lax.dot_general(eye, ref[rows, :], (((1,), (1,)), ((), ())), preferred_element_type=f32).astype(bf16)

    for k, out in enumerate((s0, s1)):
        p = (y + k) % 2
        at_head = pl.ds(pl.multiple_of(p * HEAD, HEAD), HEAD)
        out[0:32, :256] = key[:, at_head]
        out[0:32, 256:] = value[:, at_head]
        out[32:64, :256] = pool[:, at_head]
        out[32:64, 256:] = query[:, at_head]
        out[64:96, :256] = turned(pback, at_head)
        out[64:96, 256:] = turned(rback, at_head)
        s = state[p]
        hi = s.astype(bf16)
        lo = (s - hi.astype(f32)).astype(bf16)
        out[96:112, :256] = jnp.concatenate([hi, hi], axis=0)
        out[96:112, 256:] = jnp.concatenate([lo, lo], axis=0)


def pack(at, *args):
    return pl.pallas_call(
        pack_body, in_specs=[SM] + [VM] * 7, out_specs=[VM] * 2,
        out_shape=[jax.ShapeDtypeStruct((ROWS, 512), bf16)] * 2, name="pack",
    )(at, *args)


def norm_body(at, tok, gain, out, full):
    x, c = at[2], at[3]
    v = tok[...].astype(f32)
    v = v * lax.rsqrt(jnp.mean(v * v, axis=-1, keepdims=True) + eps) * gain[...]
    full[...] = v.astype(bf16)
    lane_in = lax.broadcasted_iota(jnp.int32, (256, 256), 0)
    lane_out = lax.broadcasted_iota(jnp.int32, (256, 256), 1)
    source = (lane_out % 64) // 32 * 128 + (x + NX - lane_out // 64) % NX * 32 + lane_out % 32
    order = (lane_in == source).astype(bf16)
    for zs in range(NZ):
        part = full[:, pl.ds(pl.multiple_of(zs * 512 + c * 256, 256), 256)]
        out[zs] = jnp.dot(part, order, preferred_element_type=f32).astype(bf16)


def norm(at, tok, gain):
    return pl.pallas_call(
        norm_body, in_specs=[SM, VM, VM], out_specs=VM,
        out_shape=jax.ShapeDtypeStruct((NZ, HALF, 256), bf16),
        scratch_shapes=[pltpu.VMEM((HALF, 4096), bf16)], name="norm",
    )(at, tok, gain)


def split_body(*refs):
    ins, kv, pq, sem = refs[:NZ], refs[NZ], refs[NZ + 1], refs[NZ + 2]
    copies = []
    for kz in range(NZ):
        copies.append(pltpu.make_async_copy(ins[kz].at[pl.ds(0, 64)], kv.at[pl.ds(kz * 64, 64)], sem.at[2 * kz]))
        copies.append(pltpu.make_async_copy(ins[kz].at[pl.ds(64, 64)], pq.at[pl.ds(kz * 64, 64)], sem.at[2 * kz + 1]))
    for cp in copies:
        cp.start()
    for cp in copies:
        cp.wait()


def split(chunks):
    return pl.pallas_call(
        split_body, in_specs=[ANY] * NZ, out_specs=[ANY] * 2,
        out_shape=[jax.ShapeDtypeStruct((512, 512), bf16)] * 2,
        scratch_shapes=[pltpu.SemaphoreType.DMA((2 * NZ,))], name="split",
    )(*chunks)


def project_body(at, t0, t1, t2, t3, w0, w1, w2, w3, out, lhs, rhs):
    z, y = at[0], at[1]
    for k, t in enumerate((t0, t1, t2, t3)):
        rows = pl.ds(pl.multiple_of(((y + NY - k) % NY) * HALF, HALF), HALF)
        for kz in range(NZ):
            lhs[rows, kz * 256:(kz + 1) * 256] = t[(z + kz) % NZ]
    for kx, w in enumerate((w0, w1, w2, w3)):
        for k in range(2):
            par = (y + k) % 2
            for kz in range(NZ):
                rhs[pl.ds(pl.multiple_of(kz * 256 + kx * 64 + par * 32, 32), 32), :] = w[kz * 64 + k * 32:kz * 64 + k * 32 + 32, :]
    out[...] = jnp.dot(lhs[...], rhs[...], preferred_element_type=f32)


def project(at, toks, ws):
    return pl.pallas_call(
        project_body, in_specs=[SM] + [VM] * 8, out_specs=VM,
        out_shape=jax.ShapeDtypeStruct((SPAN, 512), f32),
        scratch_shapes=[pltpu.VMEM((SPAN, 2048), bf16), pltpu.VMEM((2048, 512), bf16)],
    )(at, *toks, *ws)


def back_body(at, act, *refs):
    z, y, x = at[0], at[1], at[2]
    ws, outs, rhs = refs[:9], refs[9:13], refs[13]

    def place(ref, first, kz, kx):
        for k in range(2):
            rhs[(z + kz) % NZ, (y + k) % 2, (x + NX - kx) % NX] = ref[first + k * 32:first + k * 32 + 32, :]

    for i, kz in enumerate((0, 1, 2, 3, 5, 6, 7)):
        for kx in range(NX):
            place(ws[i], kx * 64, kz, kx)
    for kx in range(NX):
        place(ws[7 + kx // 2], (kx % 2) * 64, 4, kx)
    wt = rhs[...].reshape(2048, SPAN)
    for k, o in enumerate(outs):
        rows = act[pl.ds(pl.multiple_of(((y + k) % NY) * HALF, HALF), HALF), :]
        o[...] = lax.dot_general(rows, wt, (((1,), (1,)), ((), ())), preferred_element_type=f32).astype(bf16)


def back(at, act, ws):
    return pl.pallas_call(
        back_body, in_specs=[SM] + [VM] * 10, out_specs=[VM] * 4,
        out_shape=[jax.ShapeDtypeStruct((HALF, 2048), bf16)] * 4,
        scratch_shapes=[pltpu.VMEM((NZ, 2, NX, 32, SPAN), bf16)], name="back",
    )(at, act, *ws)


def layer(tokens, norm_gain, pool_proj, query_proj, key_proj, value_proj, pool_map, pool_scale,
          decay_rate, start_state, pool_back, retention_back):
    z, y, x, c = (lax.axis_index(a) for a in ("z", "y", "x", "c"))
    at = jnp.stack([z, y, x, c]).astype(jnp.int32)

    s0, s1 = pack(at, pool_proj, query_proj, key_proj, value_proj, start_state[0], pool_back, retention_back)
    r0 = lax.ppermute(s0, ("y", "c"), to_heads(0))
    r1 = lax.ppermute(s1, ("y", "c"), to_heads(1))
    shard_in = jnp.concatenate([r0[:32], r1[:32], r0[32:64], r1[32:64], r0[96:104], r1[96:104]], axis=0)
    shard_out = jnp.concatenate([r0[64:96], r1[64:96]], axis=0)

    toks = direct(norm(at, tokens[0], norm_gain[None]), "y", NY)

    in_z = z_ring(shard_in)
    in_z[4] = lax.ppermute(in_z[5], "z", ring(NZ, 1))
    plane_kv, plane_pq = split(in_z)
    kv_list = direct(plane_kv, "x", NX)
    pq_list = direct(plane_pq, "x", NX)

    plane_o = jnp.concatenate(direct(shard_out, "x", NX), axis=0)
    o = z_ring(plane_o)
    half_up = lax.ppermute(o[5][:128], "z", ring(NZ, 1))
    half_down = lax.ppermute(o[3][128:], "z", ring(NZ, -1))
    o_list = o[:4] + o[5:] + [half_up, half_down]

    st = jnp.stack([b[128:] for b in in_z]).reshape(NZ, 2, 8, 512)
    st = (st[..., :256].astype(f32) + st[..., 256:].astype(f32))
    st = jnp.where(y % 2 == 0, st, st[:, ::-1]).reshape(NZ, 2, 8, 2, HALF)
    keep = lax.dynamic_index_in_dim(st, c, 3, keepdims=False)
    give = lax.dynamic_index_in_dim(st, 1 - c, 3, keepdims=False)
    got = swap(give)
    both = jnp.where(c == 0, jnp.stack([keep, got], 1), jnp.stack([got, keep], 1))
    start = jnp.roll(both.reshape(NZ, 32, HALF), z, axis=0).reshape(HEAD, HALF)

    rates = jnp.where(c == y // 2, decay_rate, swap(decay_rate))
    rate = jnp.where(y % 2 == 0, rates[0], rates[1])
    scale = lax.dynamic_slice_in_dim(pool_scale, y * HEAD, HEAD, 0)
    group_map = lax.dynamic_index_in_dim(pool_map, y, 0, keepdims=False)

    within = jnp.arange(SPAN, dtype=f32)
    positions = (jnp.arange(SPAN, dtype=jnp.int32) + z * SPAN)
    inv_freq = 1.0 / rope_base ** jnp.linspace(0.0, 1.0, HALF, dtype=f32)
    angles = positions.astype(f32)[:, None] * inv_freq[None, :]
    cosine, sine = jnp.cos(angles), jnp.sin(angles)
    distance = within[:, None] - within[None, :]
    mask = jnp.where(distance >= 0, jnp.exp(-jnp.maximum(distance, 0.0) * rate), 0.0)
    key_decay = jnp.exp(-(SPAN - 1.0 - within) * rate)[:, None]
    query_decay = jnp.exp(-(within + 1.0) * rate)[:, None]
    span_decay = jnp.exp(-SPAN * rate)

    def rotate(v):
        a, b = v[:, :HALF], v[:, HALF:]
        return jnp.concatenate([a * cosine - b * sine, a * sine + b * cosine], axis=1)

    own = project(at, toks, kv_list)
    v_own = own[:, 256:].reshape(SPAN, 2, HALF)
    v_give = lax.dynamic_index_in_dim(v_own, 1 - c, 1, keepdims=False)
    v_keep = lax.dynamic_index_in_dim(v_own, c, 1, keepdims=False)
    got = swap(jnp.concatenate([own[:, :256], v_give], axis=1).astype(bf16)).astype(f32)
    key = (own[:, :256] + got[:, :256]).astype(bf16).astype(f32)
    value = (v_keep + got[:, 256:]).astype(bf16)
    rk = rotate(key) * HEAD ** -0.5
    state = lax.dot_general((rk * key_decay).astype(bf16), value, (((0,), (0,)), ((), ())), preferred_element_type=f32)
    state = state + jnp.where(z == 0, span_decay, 0.0) * start
    sent = state.astype(bf16)
    n1, n2, n3 = (lax.ppermute(sent, "z", line(NZ, k)).astype(f32) for k in (1, 2, 3))
    near = n1 + span_decay * (n2 + span_decay * n3)
    far = lax.ppermute((state + span_decay * near).astype(bf16), "z", line(NZ, 4)).astype(f32)
    carried = near + span_decay * span_decay * span_decay * far + jnp.where(z == 0, 1.0, 0.0) * start

    own = project(at, toks, pq_list)
    both = own + swap(own.astype(bf16)).astype(f32)
    pool_in = both[:, :256].astype(bf16)
    rq = rotate(both[:, 256:].astype(bf16).astype(f32))
    scores = lax.dot_general(rq.astype(bf16), rk.astype(bf16), (((1,), (1,)), ((), ())), preferred_element_type=f32)
    inside = jnp.dot((scores * mask).astype(bf16), value, preferred_element_type=f32)
    across = jnp.dot((rq * query_decay).astype(bf16), carried.astype(bf16), preferred_element_type=f32)
    ret = inside + across
    other = swap(ret)
    ret = jnp.where(c == 0, jnp.concatenate([ret, other], 1), jnp.concatenate([other, ret], 1))
    ret_out = (ret * lax.rsqrt(jnp.mean(ret * ret, axis=-1, keepdims=True) + eps)).astype(bf16)

    before = lax.ppermute(pool_in[SPAN - HALO:], "z", line(NZ, 1))
    ext = jnp.concatenate([before, pool_in], axis=0).astype(f32)
    sums = ext
    chosen = None
    n = SPAN + HALO
    for g in range(4):
        w = 2 ** g
        sums = sums + jnp.concatenate([jnp.zeros((w, HEAD), f32), sums[: n - w]], axis=0)
        chosen = sums if chosen is None else jnp.where(y == g, sums, chosen)
    window = lax.shift_left(jnp.int32(2), y)
    counts = jnp.minimum(window, positions + 1).astype(f32)[:, None]
    differ = (chosen[HALO:] / counts - ext[HALO:]).astype(bf16)
    pool_out = (jnp.dot(differ, group_map, preferred_element_type=f32) * scale).astype(bf16)

    act = jnp.concatenate([pool_out, ret_out], axis=1)
    shares = back(at, act, o_list)
    total = shares[0].astype(f32)
    for k in range(1, NY):
        total = total + lax.ppermute(shares[k], "y", ring(NY, k)).astype(f32)
    total = total.astype(bf16).reshape(2, 64, 2048)
    keep = lax.dynamic_index_in_dim(total, c, 0, keepdims=False).reshape(64, NZ, 256)
    got = swap(lax.dynamic_index_in_dim(total, 1 - c, 0, keepdims=False)).reshape(64, NZ, 256)
    mixed = jnp.where(c == 0, jnp.stack([keep, got], 2), jnp.stack([got, keep], 2))
    return mixed.reshape(1, 64, 4096)


def solution(mesh):
    torus = Mesh(mesh.devices.reshape(NZ, NY, NX, 2), ("z", "y", "x", "c"))
    sp, sp_fs = ("z", "y"), ("z", "y", "x")
    placed = (
        P("x", sp, None), P(), P(sp_fs, "c"), P(sp_fs, "c"), P(sp_fs, "c"), P(sp_fs, "c"), P(), P(),
        P("c"), P("x", "c", sp, None), P("c", sp_fs), P("c", sp_fs),
    )
    return jax.shard_map(layer, mesh=torus, in_specs=placed, out_specs=P("x", ("z", "y", "c"), None), check_vma=False)
```

```python
import jax
import jax.numpy as jnp
from jax import lax
from jax.experimental import pallas as pl
from jax.experimental.pallas import tpu as pltpu
from jax.sharding import Mesh
from jax.sharding import PartitionSpec as P

NZ, NY, NX = 8, 4, 4
SPAN = 512
HALO = 16
HEAD = 256
HALF = 128
eps = 1e-06
rope_base = 10000.0

bf16 = jnp.bfloat16
f32 = jnp.float32


def ring(n, k):
    return [(i, (i + k) % n) for i in range(n)]


def line(n, k):
    return [(i, i + k) for i in range(n - k)]


def to_heads(k):
    return [(2 * y + c, 2 * (2 * c + (k + y) % 2) + y // 2) for y in range(NY) for c in range(2)]


SWAP = [(0, 1), (1, 0)]


def swap(a):
    return lax.ppermute(a, "c", SWAP)


def direct(a, axis, n):
    return [a] + [lax.ppermute(a, axis, ring(n, k)) for k in range(1, n)]


def z_ring(a, halves):
    chunks = [None] * NZ
    chunks[0] = a
    up = down = a
    for s in range(1, 4):
        up = lax.ppermute(up, "z", ring(NZ, 1))
        down = lax.ppermute(down, "z", ring(NZ, -1))
        chunks[NZ - s], chunks[s] = up, down
    if not halves:
        chunks[4] = lax.ppermute(up, "z", ring(NZ, 1))
        return chunks
    n = a.shape[0] // 2
    return chunks[:4] + chunks[5:] + [lax.ppermute(up[:n], "z", ring(NZ, 1)), lax.ppermute(down[n:], "z", ring(NZ, -1))]


VM = pl.BlockSpec(memory_space=pltpu.VMEM)
SM = pl.BlockSpec(memory_space=pltpu.SMEM)
ANY = pl.BlockSpec(memory_space=pl.ANY)
ROWS = 112


def pack_body(at, pool, query, key, value, state, pback, rback, s0, s1):
    y = at[1]
    eye = (lax.broadcasted_iota(jnp.int32, (32, 32), 0) == lax.broadcasted_iota(jnp.int32, (32, 32), 1)).astype(bf16)

    def turned(ref, rows):
        return lax.dot_general(eye, ref[rows, :], (((1,), (1,)), ((), ())), preferred_element_type=f32).astype(bf16)

    for k, out in enumerate((s0, s1)):
        p = (y + k) % 2
        at_head = pl.ds(pl.multiple_of(p * HEAD, HEAD), HEAD)
        out[0:32, :256] = key[:, at_head]
        out[0:32, 256:] = value[:, at_head]
        out[32:64, :256] = pool[:, at_head]
        out[32:64, 256:] = query[:, at_head]
        out[64:96, :256] = turned(pback, at_head)
        out[64:96, 256:] = turned(rback, at_head)
        s = state[p]
        hi = s.astype(bf16)
        lo = (s - hi.astype(f32)).astype(bf16)
        out[96:112, :256] = jnp.concatenate([hi, hi], axis=0)
        out[96:112, 256:] = jnp.concatenate([lo, lo], axis=0)


def pack(at, *args):
    return pl.pallas_call(
        pack_body, in_specs=[SM] + [VM] * 7, out_specs=[VM] * 2,
        out_shape=[jax.ShapeDtypeStruct((ROWS, 512), bf16)] * 2, name="pack",
    )(at, *args)


def norm_body(at, tok, gain, out, full):
    x, c = at[2], at[3]
    v = tok[...].astype(f32)
    v = v * lax.rsqrt(jnp.mean(v * v, axis=-1, keepdims=True) + eps) * gain[...]
    full[...] = v.astype(bf16)
    lane_in = lax.broadcasted_iota(jnp.int32, (256, 256), 0)
    lane_out = lax.broadcasted_iota(jnp.int32, (256, 256), 1)
    source = (lane_out % 64) // 32 * 128 + (x + NX - lane_out // 64) % NX * 32 + lane_out % 32
    order = (lane_in == source).astype(bf16)
    for zs in range(NZ):
        part = full[:, pl.ds(pl.multiple_of(zs * 512 + c * 256, 256), 256)]
        out[zs] = jnp.dot(part, order, preferred_element_type=f32).astype(bf16)


def norm(at, tok, gain):
    return pl.pallas_call(
        norm_body, in_specs=[SM, VM, VM], out_specs=VM,
        out_shape=jax.ShapeDtypeStruct((NZ, HALF, 256), bf16),
        scratch_shapes=[pltpu.VMEM((HALF, 4096), bf16)], name="norm",
    )(at, tok, gain)


def split_body(at, *refs):
    z, y, c = at[0], at[1], at[3]
    ins, (kv, pq, keep, give) = refs[:NZ], refs[NZ:]
    for kz in range(NZ):
        kv[kz * 64:kz * 64 + 64, :] = ins[kz][0:64, :]
        pq[kz * 64:kz * 64 + 64, :] = ins[kz][64:128, :]
        for out, half in ((keep, c), (give, 1 - c)):
            hi = ins[kz][128:144, pl.ds(pl.multiple_of(half * HALF, HALF), HALF)].astype(f32)
            lo = ins[kz][128:144, pl.ds(pl.multiple_of(HEAD + half * HALF, HALF), HALF)].astype(f32)
            rows = hi + lo
            for k in range(2):
                at_row = ((z + kz) % NZ) * 16 + ((y + k) % 2) * 8
                out[pl.ds(pl.multiple_of(at_row, 8), 8), :] = rows[k * 8:k * 8 + 8]


def split(at, chunks):
    return pl.pallas_call(
        split_body, in_specs=[SM] + [VM] * NZ, out_specs=[VM] * 4,
        out_shape=[jax.ShapeDtypeStruct((512, 512), bf16)] * 2 + [jax.ShapeDtypeStruct((HALF, HALF), f32)] * 2,
        name="split",
    )(at, *chunks)


def lhs_body(at, t0, t1, t2, t3, out):
    z, y = at[0], at[1]
    for k, t in enumerate((t0, t1, t2, t3)):
        rows = pl.ds(pl.multiple_of(((y + NY - k) % NY) * HALF, HALF), HALF)
        for kz in range(NZ):
            out[rows, kz * 256:(kz + 1) * 256] = t[(z + kz) % NZ]


def gather_rows(at, toks):
    return pl.pallas_call(
        lhs_body, in_specs=[SM] + [VM] * 4, out_specs=VM,
        out_shape=jax.ShapeDtypeStruct((SPAN, 2048), bf16), name="rows",
    )(at, *toks)


def place_in(y, ws, rhs):
    for kx, w in enumerate(ws):
        for k in range(2):
            par = (y + k) % 2
            for kz in range(NZ):
                rhs[pl.ds(pl.multiple_of(kz * 256 + kx * 64 + par * 32, 32), 32), :] = w[kz * 64 + k * 32:kz * 64 + k * 32 + 32, :]


def kv_body(at, lhs, w0, w1, w2, w3, kpart, vkeep, send, rhs, res):
    y, c = at[1], at[3]
    place_in(y, (w0, w1, w2, w3), rhs)
    res[...] = jnp.dot(lhs[...], rhs[...], preferred_element_type=f32)
    kpart[...] = res[:, :256]
    vkeep[...] = res[:, pl.ds(pl.multiple_of(HEAD + c * HALF, HALF), HALF)]
    send[:, :256] = res[:, :256].astype(bf16)
    send[:, 256:] = res[:, pl.ds(pl.multiple_of(HEAD + (1 - c) * HALF, HALF), HALF)].astype(bf16)


def project_kv(at, lhs, ws):
    return pl.pallas_call(
        kv_body, in_specs=[SM] + [VM] * 5, out_specs=[VM] * 3,
        out_shape=[jax.ShapeDtypeStruct((SPAN, HEAD), f32), jax.ShapeDtypeStruct((SPAN, HALF), f32),
                   jax.ShapeDtypeStruct((SPAN, 384), bf16)],
        scratch_shapes=[pltpu.VMEM((2048, 512), bf16), pltpu.VMEM((SPAN, 512), f32)], name="project_kv",
    )(at, lhs, *ws)


def pq_body(at, lhs, w0, w1, w2, w3, own, send, rhs):
    place_in(at[1], (w0, w1, w2, w3), rhs)
    r = jnp.dot(lhs[...], rhs[...], preferred_element_type=f32)
    own[...] = r
    send[...] = r.astype(bf16)


def project_pq(at, lhs, ws):
    return pl.pallas_call(
        pq_body, in_specs=[SM] + [VM] * 5, out_specs=[VM] * 2,
        out_shape=[jax.ShapeDtypeStruct((SPAN, 512), f32), jax.ShapeDtypeStruct((SPAN, 512), bf16)],
        scratch_shapes=[pltpu.VMEM((2048, 512), bf16)], name="project_pq",
    )(at, lhs, *ws)


def turn(v, cosine, sine):
    a, b = v[:, :HALF], v[:, HALF:]
    return jnp.concatenate([a * cosine - b * sine, a * sine + b * cosine], axis=1)


def state_body(at, rates, kpart, vkeep, got, cosine, sine, keep, other, rk, val, state, sent, start):
    z, c = at[0], at[3]
    for zs in range(NZ):
        start[pl.ds(pl.multiple_of(zs * 32 + c * 16, 16), 16), :] = keep[zs * 16:zs * 16 + 16, :]
        start[pl.ds(pl.multiple_of(zs * 32 + (1 - c) * 16, 16), 16), :] = other[zs * 16:zs * 16 + 16, :]
    key = (kpart[...] + got[:, :256].astype(f32)).astype(bf16).astype(f32)
    value = (vkeep[...] + got[:, 256:].astype(f32)).astype(bf16)
    val[...] = value
    turned = turn(key, cosine[...], sine[...]) * HEAD ** -0.5
    rk[...] = turned.astype(bf16)
    within = lax.broadcasted_iota(jnp.int32, (SPAN, HEAD), 0).astype(f32)
    faded = (turned * jnp.exp(-(SPAN - 1.0 - within) * rates[0])).astype(bf16)
    s = lax.dot_general(faded, value, (((0,), (0,)), ((), ())), preferred_element_type=f32)
    s = s + jnp.where(z == 0, rates[1], 0.0) * start[...]
    state[...] = s
    sent[...] = s.astype(bf16)


def span_state(at, rates, *args):
    return pl.pallas_call(
        state_body, in_specs=[SM, SM] + [VM] * 7, out_specs=[VM] * 5,
        out_shape=[jax.ShapeDtypeStruct((SPAN, HEAD), bf16), jax.ShapeDtypeStruct((SPAN, HALF), bf16),
                   jax.ShapeDtypeStruct((HEAD, HALF), f32), jax.ShapeDtypeStruct((HEAD, HALF), bf16),
                   jax.ShapeDtypeStruct((HEAD, HALF), f32)],
        name="span_state",
    )(at, rates, *args)


def inside_body(rates, own, got, cosine, sine, rk, val, pool_in, inside, faded):
    pool_in[...] = (own[:, :256] + got[:, :256].astype(f32)).astype(bf16)
    query = (own[:, 256:] + got[:, 256:].astype(f32)).astype(bf16).astype(f32)
    rq = turn(query, cosine[...], sine[...])
    within = lax.broadcasted_iota(jnp.int32, (SPAN, HEAD), 0).astype(f32)
    faded[...] = (rq * jnp.exp(-(within + 1.0) * rates[0])).astype(bf16)
    rq = rq.astype(bf16)
    for b in range(4):
        n = (b + 1) * 128
        scores = lax.dot_general(rq[b * 128:n], rk[:n, :], (((1,), (1,)), ((), ())), preferred_element_type=f32)
        far = lax.broadcasted_iota(jnp.int32, (128, n), 0) + b * 128 - lax.broadcasted_iota(jnp.int32, (128, n), 1)
        fade = jnp.exp(-jnp.maximum(far, 0).astype(f32) * rates[0])
        weights = jnp.where(far >= 0, scores * fade, 0.0).astype(bf16)
        inside[b * 128:n, :] = jnp.dot(weights, val[:n, :], preferred_element_type=f32)


def inside_span(rates, *args):
    return pl.pallas_call(
        inside_body, in_specs=[SM] + [VM] * 6, out_specs=[VM] * 3,
        out_shape=[jax.ShapeDtypeStruct((SPAN, HEAD), bf16), jax.ShapeDtypeStruct((SPAN, HALF), f32),
                   jax.ShapeDtypeStruct((SPAN, HEAD), bf16)],
        name="inside",
    )(rates, *args)


def across_body(at, rates, inside, faded, near, far, start, ret):
    d = rates[1]
    carried = near[...] + d * d * d * far[...].astype(f32) + jnp.where(at[0] == 0, 1.0, 0.0) * start[...]
    ret[...] = inside[...] + jnp.dot(faded[...], carried.astype(bf16), preferred_element_type=f32)


def across_spans(at, rates, *args):
    return pl.pallas_call(
        across_body, in_specs=[SM, SM] + [VM] * 5, out_specs=VM,
        out_shape=jax.ShapeDtypeStruct((SPAN, HALF), f32), name="across",
    )(at, rates, *args)


def pool_body(at, pool_in, before, group_map, scale, out):
    z, y = at[0], at[1]
    ext = jnp.concatenate([before[...], pool_in[...]], axis=0).astype(f32)
    sums = ext
    chosen = None
    for g in range(4):
        sums = sums + pltpu.roll(sums, 2 ** g, 0)
        chosen = sums if chosen is None else jnp.where(y == g, sums, chosen)
    rows = lax.broadcasted_iota(jnp.int32, (SPAN, HEAD), 0) + z * SPAN + 1
    counts = jnp.minimum(lax.shift_left(jnp.int32(2), y), rows).astype(f32)
    differ = (chosen[HALO:] / counts - ext[HALO:]).astype(bf16)
    out[...] = (jnp.dot(differ, group_map[...], preferred_element_type=f32) * scale[...]).astype(bf16)


def pooling(at, *args):
    return pl.pallas_call(
        pool_body, in_specs=[SM] + [VM] * 4, out_specs=VM,
        out_shape=jax.ShapeDtypeStruct((SPAN, HEAD), bf16), name="pooling",
    )(at, *args)


def arrange_body(at, *refs):
    z, y, x = at[0], at[1], at[2]
    ws, out = refs[:9], refs[9]

    def place(ref, first, kz, kx):
        for k in range(2):
            row = ((z + kz) % NZ) * 256 + ((y + k) % 2) * 128 + ((x + NX - kx) % NX) * 32
            out[pl.ds(pl.multiple_of(row, 32), 32), :] = ref[first + k * 32:first + k * 32 + 32, :]

    for i, kz in enumerate((0, 1, 2, 3, 5, 6, 7)):
        for kx in range(NX):
            place(ws[i], kx * 64, kz, kx)
    for kx in range(NX):
        place(ws[7 + kx // 2], (kx % 2) * 64, 4, kx)


def arrange(at, ws):
    return pl.pallas_call(
        arrange_body, in_specs=[SM] + [VM] * 9, out_specs=VM,
        out_shape=jax.ShapeDtypeStruct((2048, SPAN), bf16), name="arrange",
    )(at, *ws)


def back_body(at, pool, ret, other, wt, o0, o1, o2, o3, act, res):
    y, c = at[1], at[3]
    r, o = ret[...], other[...]
    square = jnp.sum(r * r, axis=-1, keepdims=True) + jnp.sum(o * o, axis=-1, keepdims=True)
    factor = lax.rsqrt(square * (1.0 / HEAD) + eps)
    act[:, :256] = pool[...]
    act[:, pl.ds(pl.multiple_of(HEAD + c * HALF, HALF), HALF)] = (r * factor).astype(bf16)
    act[:, pl.ds(pl.multiple_of(HEAD + (1 - c) * HALF, HALF), HALF)] = (o * factor).astype(bf16)
    res[...] = lax.dot_general(act[...], wt[...], (((1,), (1,)), ((), ())), preferred_element_type=f32).astype(bf16)
    for k, out in enumerate((o0, o1, o2, o3)):
        out[...] = res[pl.ds(pl.multiple_of(((y + k) % NY) * HALF, HALF), HALF), :]


def back(at, *args):
    return pl.pallas_call(
        back_body, in_specs=[SM] + [VM] * 4, out_specs=[VM] * 4,
        out_shape=[jax.ShapeDtypeStruct((HALF, 2048), bf16)] * 4,
        scratch_shapes=[pltpu.VMEM((SPAN, 512), bf16), pltpu.VMEM((SPAN, 2048), bf16)], name="back",
    )(at, *args)


def layer(tokens, norm_gain, pool_proj, query_proj, key_proj, value_proj, pool_map, pool_scale,
          decay_rate, start_state, pool_back, retention_back):
    z, y, x, c = (lax.axis_index(a) for a in ("z", "y", "x", "c"))
    at = jnp.stack([z, y, x, c]).astype(jnp.int32)

    s0, s1 = pack(at, pool_proj, query_proj, key_proj, value_proj, start_state[0], pool_back, retention_back)
    r0 = lax.ppermute(s0, ("y", "c"), to_heads(0))
    r1 = lax.ppermute(s1, ("y", "c"), to_heads(1))
    shard_in = jnp.concatenate([r0[:32], r1[:32], r0[32:64], r1[32:64], r0[96:104], r1[96:104]], axis=0)
    shard_out = jnp.concatenate([r0[64:96], r1[64:96]], axis=0)

    toks = direct(norm(at, tokens[0], norm_gain[None]), "y", NY)

    lhs = gather_rows(at, toks)

    in_z = z_ring(shard_in, False)
    plane_kv, plane_pq, keep, give = split(at, in_z)
    kv_list = direct(plane_kv, "x", NX)
    pq_list = direct(plane_pq, "x", NX)
    start_other = swap(give)

    plane_o = jnp.concatenate(direct(shard_out, "x", NX), axis=0)
    wt = arrange(at, z_ring(plane_o, True))

    decays = jnp.where(c == y // 2, decay_rate, swap(decay_rate))
    rate = jnp.where(y % 2 == 0, decays[0], decays[1])
    span_decay = jnp.exp(-SPAN * rate)
    rates = jnp.stack([rate, span_decay])
    scale = lax.dynamic_slice_in_dim(pool_scale, y * HEAD, HEAD, 0)[None]
    group_map = lax.dynamic_index_in_dim(pool_map, y, 0, keepdims=False)
    positions = (jnp.arange(SPAN, dtype=jnp.int32) + z * SPAN)
    inv_freq = 1.0 / rope_base ** jnp.linspace(0.0, 1.0, HALF, dtype=f32)
    angles = positions.astype(f32)[:, None] * inv_freq[None, :]
    cosine, sine = jnp.cos(angles), jnp.sin(angles)

    kpart, vkeep, send = project_kv(at, lhs, kv_list)
    got = swap(send)
    rk, val, state, sent, start = span_state(at, rates, kpart, vkeep, got, cosine, sine, keep, start_other)
    n1, n2, n3 = (lax.ppermute(sent, "z", line(NZ, k)).astype(f32) for k in (1, 2, 3))
    near = n1 + span_decay * (n2 + span_decay * n3)
    far = lax.ppermute((state + span_decay * near).astype(bf16), "z", line(NZ, 4))

    own, send = project_pq(at, lhs, pq_list)
    got = swap(send)
    pool_in, inside, faded = inside_span(rates, own, got, cosine, sine, rk, val)
    before = lax.ppermute(pool_in[SPAN - HALO:], "z", line(NZ, 1))
    pool_out = pooling(at, pool_in, before, group_map, scale)
    ret = across_spans(at, rates, inside, faded, near, far, start)
    other = swap(ret)

    shares = back(at, pool_out, ret, other, wt)
    total = shares[0].astype(f32)
    for k in range(1, NY):
        total = total + lax.ppermute(shares[k], "y", ring(NY, k)).astype(f32)
    total = total.astype(bf16).reshape(2, 64, 2048)
    keep = lax.dynamic_index_in_dim(total, c, 0, keepdims=False).reshape(64, NZ, 256)
    got = swap(lax.dynamic_index_in_dim(total, 1 - c, 0, keepdims=False)).reshape(64, NZ, 256)
    mixed = jnp.where(c == 0, jnp.stack([keep, got], 2), jnp.stack([got, keep], 2))
    return mixed.reshape(1, 64, 4096)


def solution(mesh):
    torus = Mesh(mesh.devices.reshape(NZ, NY, NX, 2), ("z", "y", "x", "c"))
    sp, sp_fs = ("z", "y"), ("z", "y", "x")
    placed = (
        P("x", sp, None), P(), P(sp_fs, "c"), P(sp_fs, "c"), P(sp_fs, "c"), P(sp_fs, "c"), P(), P(),
        P("c"), P("x", "c", sp, None), P("c", sp_fs), P("c", sp_fs),
    )
    return jax.shard_map(layer, mesh=torus, in_specs=placed, out_specs=P("x", ("z", "y", "c"), None), check_vma=False)
```

```python
import jax
import jax.numpy as jnp
from jax import lax
from jax.experimental import pallas as pl
from jax.experimental.pallas import tpu as pltpu
from jax.sharding import Mesh
from jax.sharding import PartitionSpec as P

NZ, NY, NX = 8, 4, 4
SPAN = 512
HALO = 16
HEAD = 256
HALF = 128
eps = 1e-06
rope_base = 10000.0

bf16 = jnp.bfloat16
f32 = jnp.float32


def ring(n, k):
    return [(i, (i + k) % n) for i in range(n)]


def line(n, k):
    return [(i, i + k) for i in range(n - k)]


def to_heads(k):
    return [(2 * y + c, 2 * (2 * c + (k + y) % 2) + y // 2) for y in range(NY) for c in range(2)]


SWAP = [(0, 1), (1, 0)]


def swap(a):
    return lax.ppermute(a, "c", SWAP)


def direct(a, axis, n):
    return [a] + [lax.ppermute(a, axis, ring(n, k)) for k in range(1, n)]


def x_ring(a):
    n = a.shape[0] // 2
    one = lax.ppermute(a, "x", ring(NX, 1))
    three = lax.ppermute(a, "x", ring(NX, -1))
    top = lax.ppermute(one[:n], "x", ring(NX, 1))
    low = lax.ppermute(three[n:], "x", ring(NX, -1))
    return [a, one, top, low, three]


def z_ring(a, halves):
    chunks = [None] * NZ
    chunks[0] = a
    up = down = a
    for s in range(1, 4):
        up = lax.ppermute(up, "z", ring(NZ, 1))
        down = lax.ppermute(down, "z", ring(NZ, -1))
        chunks[NZ - s], chunks[s] = up, down
    if not halves:
        chunks[4] = lax.ppermute(up, "z", ring(NZ, 1))
        return chunks
    n = a.shape[0] // 2
    return chunks[:4] + chunks[5:] + [lax.ppermute(up[:n], "z", ring(NZ, 1)), lax.ppermute(down[n:], "z", ring(NZ, -1))]


VM = pl.BlockSpec(memory_space=pltpu.VMEM)
SM = pl.BlockSpec(memory_space=pltpu.SMEM)
ANY = pl.BlockSpec(memory_space=pl.ANY)


def local(body, **kw):
    return pl.pallas_call(body, compiler_params=pltpu.CompilerParams(vmem_limit_bytes=16 * 2**20), **kw)


ROWS = 112


def pack_body(at, decay, pool, query, key, value, state, pback, rback, s0, s1):
    y = at[1]
    for k, out in enumerate((s0, s1)):
        p = (y + k) % 2
        at_head = pl.ds(pl.multiple_of(p * HEAD, HEAD), HEAD)
        out[0:32, :256] = key[:, at_head]
        out[0:32, 256:] = value[:, at_head]
        out[32:64, :256] = pool[:, at_head]
        out[32:64, 256:] = query[:, at_head]
        out[64:96, :256] = pback[:, at_head]
        out[64:96, 256:] = rback[:, at_head]
        s = state[p]
        hi = s.astype(bf16)
        lo = (s - hi.astype(f32)).astype(bf16)
        d = jnp.full((8, HALF), decay[p], f32)
        d1 = d.astype(bf16)
        d2 = (d - d1.astype(f32)).astype(bf16)
        d3 = (d - d1.astype(f32) - d2.astype(f32)).astype(bf16)
        out[96:112, :256] = jnp.concatenate([hi, jnp.concatenate([d1, d2], axis=1)], axis=0)
        out[96:112, 256:] = jnp.concatenate([lo, jnp.concatenate([d3, d3], axis=1)], axis=0)


def pack(at, *args):
    return local(
        pack_body, in_specs=[SM, SM] + [VM] * 7, out_specs=[VM] * 2,
        out_shape=[jax.ShapeDtypeStruct((ROWS, 512), bf16)] * 2, name="pack",
    )(at, *args)


def norm_body(at, tok, gain, out, full):
    z, x, c = at[0], at[2], at[3]
    v = tok[...].astype(f32)
    v = v * lax.rsqrt(jnp.mean(v * v, axis=-1, keepdims=True) + eps) * gain[...]
    full[...] = v.astype(bf16)
    lane_in = lax.broadcasted_iota(jnp.int32, (512, 512), 0)
    lane_out = lax.broadcasted_iota(jnp.int32, (512, 512), 1)
    source = (lane_out % 128) // 64 * 256 + (lane_out % 64) // 32 * 128 + (x + NX - lane_out // 128) % NX * 32 + lane_out % 32
    order = (lane_in == source).astype(bf16)
    for pair in range(NZ // 2):
        two = [full[:, pl.ds(pl.multiple_of((z + 2 * pair + i) % NZ * 512 + c * 256, 256), 256)] for i in range(2)]
        r = jnp.dot(jnp.concatenate(two, axis=1), order, preferred_element_type=f32).astype(bf16)
        for kx in range(NX):
            out[kx, :, pair * 128:pair * 128 + 128] = r[:, kx * 128:kx * 128 + 128]


def norm(at, tok, gain):
    return local(
        norm_body, in_specs=[SM, VM, VM], out_specs=VM,
        out_shape=jax.ShapeDtypeStruct((NX, HALF, 512), bf16),
        scratch_shapes=[pltpu.VMEM((HALF, 4096), bf16)], name="norm",
    )(at, tok, gain)


def split_kv_body(*refs):
    for kz in range(NZ):
        refs[NZ][kz * 64:kz * 64 + 64, :] = refs[kz][0:64, :]


def split_kv(chunks):
    return local(
        split_kv_body, in_specs=[VM] * NZ, out_specs=VM,
        out_shape=jax.ShapeDtypeStruct((512, 512), bf16), name="split_kv",
    )(*chunks)


def split_pq_body(at, *refs):
    z, c = at[0], at[3]
    ins, (pq, keep, give) = refs[:NZ], refs[NZ:]
    for kz in range(NZ):
        pq[kz * 64:kz * 64 + 64, :] = ins[kz][64:128, :]
        for out, half in ((keep, c), (give, 1 - c)):
            hi = ins[kz][128:144, pl.ds(pl.multiple_of(half * HALF, HALF), HALF)].astype(f32)
            lo = ins[kz][128:144, pl.ds(pl.multiple_of(HEAD + half * HALF, HALF), HALF)].astype(f32)
            out[pl.ds(pl.multiple_of(((z + kz) % NZ) * 16, 16), 16), :] = hi + lo


def split_pq(at, chunks):
    return local(
        split_pq_body, in_specs=[SM] + [VM] * NZ, out_specs=[VM] * 3,
        out_shape=[jax.ShapeDtypeStruct((512, 512), bf16)] + [jax.ShapeDtypeStruct((HALF, HALF), f32)] * 2,
        name="split_pq",
    )(at, *chunks)


def multiply(toks, ws):
    w0, w1, w2a, w2b, w3 = ws
    acc = None
    for kx in range(NX):
        w = jnp.concatenate([w2a[...], w2b[...]], axis=0) if kx == 2 else (w0, w1, None, w3)[kx][...]
        rows = jnp.concatenate([t[kx] for t in toks], axis=0)
        r = jnp.dot(rows, w, preferred_element_type=f32)
        acc = r if acc is None else acc + r
    return acc


def span_rows(y, k):
    return pl.ds(pl.multiple_of(((y + NY - k) % NY) * HALF, HALF), HALF)


def kv_body(at, *refs):
    y, c = at[1], at[3]
    toks, ws, (kpart, vkeep, send) = refs[:4], refs[4:9], refs[9:]
    acc = multiply(toks, ws)
    for k in range(NY):
        r = acc[k * HALF:(k + 1) * HALF]
        rows = span_rows(y, k)
        kpart[rows, :] = r[:, :256]
        vkeep[rows, :] = jnp.where(c == 0, r[:, 256:384], r[:, 384:])
        send[rows, :256] = r[:, :256].astype(bf16)
        send[rows, 256:] = jnp.where(c == 0, r[:, 384:], r[:, 256:384]).astype(bf16)


def project_kv(at, toks, ws):
    return local(
        kv_body, in_specs=[SM] + [VM] * 9, out_specs=[VM] * 3,
        out_shape=[jax.ShapeDtypeStruct((SPAN, HEAD), f32), jax.ShapeDtypeStruct((SPAN, HALF), f32),
                   jax.ShapeDtypeStruct((SPAN, 384), bf16)],
        name="project_kv",
    )(at, *toks, *ws)


def pq_body(at, *refs):
    toks, ws, (own, send) = refs[:4], refs[4:9], refs[9:]
    acc = multiply(toks, ws)
    for k in range(NY):
        r = acc[k * HALF:(k + 1) * HALF]
        rows = span_rows(at[1], k)
        own[rows, :] = r
        send[rows, :] = r.astype(bf16)


def project_pq(at, toks, ws):
    return local(
        pq_body, in_specs=[SM] + [VM] * 9, out_specs=[VM] * 2,
        out_shape=[jax.ShapeDtypeStruct((SPAN, 512), f32), jax.ShapeDtypeStruct((SPAN, 512), bf16)],
        name="project_pq",
    )(at, *toks, *ws)


def turn(v, cosine, sine):
    a, b = v[:, :HALF], v[:, HALF:]
    return jnp.concatenate([a * cosine - b * sine, a * sine + b * cosine], axis=1)


def state_body(at, rates, kpart, vkeep, got, cosine, sine, keep, other, rk, val, state, sent, start):
    z, c = at[0], at[3]
    for zs in range(NZ):
        start[pl.ds(pl.multiple_of(zs * 32 + c * 16, 16), 16), :] = keep[zs * 16:zs * 16 + 16, :]
        start[pl.ds(pl.multiple_of(zs * 32 + (1 - c) * 16, 16), 16), :] = other[zs * 16:zs * 16 + 16, :]
    key = (kpart[...] + got[:, :256].astype(f32)).astype(bf16).astype(f32)
    value = (vkeep[...] + got[:, 256:].astype(f32)).astype(bf16)
    val[...] = value
    turned = turn(key, cosine[...], sine[...]) * HEAD ** -0.5
    rk[...] = turned.astype(bf16)
    within = lax.broadcasted_iota(jnp.int32, (SPAN, HALF), 0).astype(f32)
    fade = jnp.exp(-(SPAN - 1.0 - within) * rates[0:1, :])
    faded = (turned * jnp.concatenate([fade, fade], axis=1)).astype(bf16)
    s = lax.dot_general(faded, value, (((0,), (0,)), ((), ())), preferred_element_type=f32)
    s = s + jnp.where(z == 0, rates[8:9, :], 0.0) * start[...]
    state[...] = s
    sent[...] = s.astype(bf16)


def span_state(at, rates, *args):
    return local(
        state_body, in_specs=[SM] + [VM] * 8, out_specs=[VM] * 5,
        out_shape=[jax.ShapeDtypeStruct((SPAN, HEAD), bf16), jax.ShapeDtypeStruct((SPAN, HALF), bf16),
                   jax.ShapeDtypeStruct((HEAD, HALF), f32), jax.ShapeDtypeStruct((HEAD, HALF), bf16),
                   jax.ShapeDtypeStruct((HEAD, HALF), f32)],
        name="span_state",
    )(at, rates, *args)


def inside_body(rates, own, got, cosine, sine, rk, val, pool_in, tail, inside, faded):
    p = (own[:, :256] + got[:, :256].astype(f32)).astype(bf16)
    pool_in[...] = p
    tail[...] = p[SPAN - HALO:]
    query = (own[:, 256:] + got[:, 256:].astype(f32)).astype(bf16).astype(f32)
    rq = turn(query, cosine[...], sine[...])
    within = lax.broadcasted_iota(jnp.int32, (SPAN, HALF), 0).astype(f32)
    fade = jnp.exp(-(within + 1.0) * rates[0:1, :])
    faded[...] = (rq * jnp.concatenate([fade, fade], axis=1)).astype(bf16)
    rq = rq.astype(bf16)
    for b in range(4):
        n = (b + 1) * 128
        scores = lax.dot_general(rq[b * 128:n], rk[:n, :], (((1,), (1,)), ((), ())), preferred_element_type=f32)
        far = lax.broadcasted_iota(jnp.int32, (128, n), 0) + b * 128 - lax.broadcasted_iota(jnp.int32, (128, n), 1)
        fade = jnp.exp(-jnp.maximum(far, 0).astype(f32) * jnp.concatenate([rates[0:1, :]] * (b + 1), axis=1))
        weights = jnp.where(far >= 0, scores * fade, 0.0).astype(bf16)
        inside[b * 128:n, :] = jnp.dot(weights, val[:n, :], preferred_element_type=f32)


def inside_span(rates, *args):
    return local(
        inside_body, in_specs=[VM] * 7, out_specs=[VM] * 4,
        out_shape=[jax.ShapeDtypeStruct((SPAN, HEAD), bf16), jax.ShapeDtypeStruct((HALO, HEAD), bf16),
                   jax.ShapeDtypeStruct((SPAN, HALF), f32),
                   jax.ShapeDtypeStruct((SPAN, HEAD), bf16)],
        name="inside",
    )(rates, *args)


def across_body(at, rates, inside, faded, near, far, start, ret):
    d = rates[8:9, :]
    carried = near[...] + d * d * d * far[...].astype(f32) + jnp.where(at[0] == 0, 1.0, 0.0) * start[...]
    ret[...] = inside[...] + jnp.dot(faded[...], carried.astype(bf16), preferred_element_type=f32)


def across_spans(at, rates, *args):
    return local(
        across_body, in_specs=[SM] + [VM] * 6, out_specs=VM,
        out_shape=jax.ShapeDtypeStruct((SPAN, HALF), f32), name="across",
    )(at, rates, *args)


def pool_body(at, pool_in, before, group_map, scale, out):
    z, y = at[0], at[1]
    ext = jnp.concatenate([before[...], pool_in[...]], axis=0).astype(f32)
    sums = ext
    chosen = None
    for g in range(4):
        sums = sums + pltpu.roll(sums, 2 ** g, 0)
        chosen = sums if chosen is None else jnp.where(y == g, sums, chosen)
    rows = lax.broadcasted_iota(jnp.int32, (SPAN, HEAD), 0) + z * SPAN + 1
    counts = jnp.minimum(lax.shift_left(jnp.int32(2), y), rows).astype(f32)
    differ = (chosen[HALO:] / counts - ext[HALO:]).astype(bf16)
    out[...] = (jnp.dot(differ, group_map[y], preferred_element_type=f32) * scale[:, pl.ds(pl.multiple_of(y * HEAD, HEAD), HEAD)]).astype(bf16)


def pooling(at, *args):
    return local(
        pool_body, in_specs=[SM] + [VM] * 4, out_specs=VM,
        out_shape=jax.ShapeDtypeStruct((SPAN, HEAD), bf16), name="pooling",
    )(at, *args)


def back_body(at, pool, ret, other, *refs):
    y, c = at[1], at[3]
    ws, outs, act, res = refs[:9], refs[9:13], refs[13], refs[14]
    r, o = ret[...], other[...]
    square = jnp.sum(r * r, axis=-1, keepdims=True) + jnp.sum(o * o, axis=-1, keepdims=True)
    factor = lax.rsqrt(square * (1.0 / HEAD) + eps)
    act[:, :256] = pool[...]
    act[:, pl.ds(pl.multiple_of(HEAD + c * HALF, HALF), HALF)] = (r * factor).astype(bf16)
    act[:, pl.ds(pl.multiple_of(HEAD + (1 - c) * HALF, HALF), HALF)] = (o * factor).astype(bf16)
    for i, kz in enumerate((0, 1, 2, 3, 5, 6, 7, 4)):
        w = ws[i][...] if kz != 4 else jnp.concatenate([ws[7][...], ws[8][...]], axis=0)
        r = lax.dot_general(act[...], w, (((1,), (1,)), ((), ())), preferred_element_type=f32)
        res[:, kz * 256:kz * 256 + 256] = r.astype(bf16)
    for k, out in enumerate(outs):
        out[...] = res[pl.ds(pl.multiple_of(((y + k) % NY) * HALF, HALF), HALF), :]


def back(at, pool, ret, other, ws):
    return local(
        back_body, in_specs=[SM] + [VM] * 12, out_specs=[VM] * 4,
        out_shape=[jax.ShapeDtypeStruct((HALF, 2048), bf16)] * 4,
        scratch_shapes=[pltpu.VMEM((SPAN, 512), bf16), pltpu.VMEM((SPAN, 2048), bf16)], name="back",
    )(at, pool, ret, other, *ws)


def total_body(at, s0, s1, s2, s3, keep, give):
    c = at[3]
    for out, half in ((keep, c), (give, 1 - c)):
        rows = pl.ds(pl.multiple_of(half * 64, 64), 64)
        out[...] = (s0[rows, :].astype(f32) + s1[rows, :].astype(f32) + (s2[rows, :].astype(f32) + s3[rows, :].astype(f32))).astype(bf16)


def total(at, arrived):
    return local(
        total_body, in_specs=[SM] + [VM] * 4, out_specs=[VM] * 2,
        out_shape=[jax.ShapeDtypeStruct((64, 2048), bf16)] * 2, name="total",
    )(at, *arrived)


def mixed_body(at, keep, got, out):
    z, x, c = at[0], at[2], at[3]
    lane_in = lax.broadcasted_iota(jnp.int32, (256, 256), 0)
    lane_out = lax.broadcasted_iota(jnp.int32, (256, 256), 1)
    source = (x + NX - (lane_out % 128) // 32) % NX * 64 + lane_out // 128 * 32 + lane_out % 32
    order = (lane_in == source).astype(bf16)
    for kz in range(NZ):
        for ref, core in ((keep, c), (got, 1 - c)):
            r = jnp.dot(ref[:, kz * 256:kz * 256 + 256], order, preferred_element_type=f32).astype(bf16)
            out[:, pl.ds(pl.multiple_of((z + kz) % NZ * 512 + core * 256, 256), 256)] = r


def mixed(at, keep, got):
    return local(
        mixed_body, in_specs=[SM] + [VM] * 2, out_specs=VM,
        out_shape=jax.ShapeDtypeStruct((64, 4096), bf16), name="mixed",
    )(at, keep, got)


def layer(tokens, norm_gain, pool_proj, query_proj, key_proj, value_proj, pool_map, pool_scale,
          decay_rate, start_state, pool_back, retention_back):
    z, y, x, c = (lax.axis_index(a) for a in ("z", "y", "x", "c"))
    at = jnp.stack([z, y, x, c]).astype(jnp.int32)

    s0, s1 = pack(at, decay_rate, pool_proj, query_proj, key_proj, value_proj, start_state[0], pool_back.T, retention_back.T)
    r0 = lax.ppermute(s0, ("y", "c"), to_heads(0))
    r1 = lax.ppermute(s1, ("y", "c"), to_heads(1))
    even = y % 2 == 0
    a, b = jnp.where(even, r0, r1), jnp.where(even, r1, r0)
    shard_in = jnp.concatenate([a[:32], b[:32], a[32:64], b[32:64], a[96:104], b[96:104]], axis=0)
    shard_out = jnp.concatenate([a[64:96], b[64:96]], axis=0)

    toks = direct(norm(at, tokens[0], norm_gain[None]), "y", NY)


    in_z = z_ring(shard_in, False)
    kv_list = x_ring(split_kv(in_z))
    plane_pq, keep, give = split_pq(at, in_z)
    pq_list = x_ring(plane_pq)
    start_other = swap(give)

    plane_o = jnp.concatenate(direct(shard_out, "x", NX), axis=0)
    wt = z_ring(plane_o, True)

    three = r0[104:112, :].astype(f32)
    rate = (three[:, :128] + three[:, 128:256]) + three[:, 256:384]
    rates = jnp.concatenate([rate, jnp.exp(-SPAN * rate)], axis=0)
    span_decay = rates[8:9, :]
    positions = (jnp.arange(SPAN, dtype=jnp.int32) + z * SPAN)
    inv_freq = 1.0 / rope_base ** jnp.linspace(0.0, 1.0, HALF, dtype=f32)
    angles = positions.astype(f32)[:, None] * inv_freq[None, :]
    cosine, sine = jnp.cos(angles), jnp.sin(angles)

    kpart, vkeep, send = project_kv(at, toks, kv_list)
    got = swap(send)
    rk, val, state, sent, start = span_state(at, rates, kpart, vkeep, got, cosine, sine, keep, start_other)
    n1, n2, n3 = (lax.ppermute(sent, "z", line(NZ, k)).astype(f32) for k in (1, 2, 3))
    near = n1 + span_decay * (n2 + span_decay * n3)
    far = lax.ppermute((state + span_decay * near).astype(bf16), "z", line(NZ, 4))

    own, send = project_pq(at, toks, pq_list)
    got = swap(send)
    pool_in, tail, inside, faded = inside_span(rates, own, got, cosine, sine, rk, val)
    before = lax.ppermute(tail, "z", line(NZ, 1))
    pool_out = pooling(at, pool_in, before, pool_map, pool_scale[None])
    ret = across_spans(at, rates, inside, faded, near, far, start)
    other = swap(ret)

    shares = back(at, pool_out, ret, other, wt)
    arrived = [shares[0]] + [lax.ppermute(shares[k], "y", ring(NY, k)) for k in range(1, NY)]
    keep, give = total(at, arrived)
    got = swap(give)
    return mixed(at, keep, got)[None]


def solution(mesh):
    torus = Mesh(mesh.devices.reshape(NZ, NY, NX, 2), ("z", "y", "x", "c"))
    sp, sp_fs = ("z", "y"), ("z", "y", "x")
    placed = (
        P("x", sp, None), P(), P(sp_fs, "c"), P(sp_fs, "c"), P(sp_fs, "c"), P(sp_fs, "c"), P(), P(),
        P("c"), P("x", "c", sp, None), P("c", sp_fs), P("c", sp_fs),
    )
    return jax.shard_map(layer, mesh=torus, in_specs=placed, out_specs=P("x", ("z", "y", "c"), None), check_vma=False)
```

```python
import jax
import jax.numpy as jnp
from jax import lax
from jax.experimental import pallas as pl
from jax.experimental.pallas import tpu as pltpu
from jax.sharding import Mesh
from jax.sharding import PartitionSpec as P

NZ, NY, NX = 8, 4, 4
SPAN = 512
HALO = 16
HEAD = 256
HALF = 128
eps = 1e-06
rope_base = 10000.0

bf16 = jnp.bfloat16
f32 = jnp.float32


def ring(n, k):
    return [(i, (i + k) % n) for i in range(n)]


def line(n, k):
    return [(i, i + k) for i in range(n - k)]


def to_heads(k):
    return [(2 * y + c, 2 * (2 * c + (k + y) % 2) + y // 2) for y in range(NY) for c in range(2)]


SWAP = [(0, 1), (1, 0)]


def swap(a):
    return lax.ppermute(a, "c", SWAP)


def direct(a, axis, n):
    return [a] + [lax.ppermute(a, axis, ring(n, k)) for k in range(1, n)]


def z_ring(a, halves):
    chunks = [None] * NZ
    chunks[0] = a
    up = down = a
    for s in range(1, 4):
        up = lax.ppermute(up, "z", ring(NZ, 1))
        down = lax.ppermute(down, "z", ring(NZ, -1))
        chunks[NZ - s], chunks[s] = up, down
    if not halves:
        chunks[4] = lax.ppermute(up, "z", ring(NZ, 1))
        return chunks
    n = a.shape[0] // 2
    return chunks[:4] + chunks[5:] + [lax.ppermute(up[:n], "z", ring(NZ, 1)), lax.ppermute(down[n:], "z", ring(NZ, -1))]


VM = pl.BlockSpec(memory_space=pltpu.VMEM)
SM = pl.BlockSpec(memory_space=pltpu.SMEM)
ANY = pl.BlockSpec(memory_space=pl.ANY)


def local(body, **kw):
    return pl.pallas_call(body, compiler_params=pltpu.CompilerParams(vmem_limit_bytes=16 * 2**20), **kw)


ROWS = 112


def pack_body(at, decay, *refs):
    y = at[1]
    sources, (s0, s1), held, sem = refs[:7], refs[7:9], refs[9:16], refs[16]
    copies = [pltpu.make_async_copy(a, b, sem.at[i]) for i, (a, b) in enumerate(zip(sources, held))]
    for cp in copies:
        cp.start()
    for cp in copies:
        cp.wait()
    pool, query, key, value, state, pback, rback = held
    for k, out in enumerate((s0, s1)):
        p = (y + k) % 2
        at_head = pl.ds(pl.multiple_of(p * HEAD, HEAD), HEAD)
        out[0:32, :256] = key[:, at_head]
        out[0:32, 256:] = value[:, at_head]
        out[32:64, :256] = pool[:, at_head]
        out[32:64, 256:] = query[:, at_head]
        out[64:96, :256] = pback[:, at_head]
        out[64:96, 256:] = rback[:, at_head]
        s = state[p]
        hi = s.astype(bf16)
        lo = (s - hi.astype(f32)).astype(bf16)
        d = jnp.full((8, HALF), decay[p], f32)
        d1 = d.astype(bf16)
        d2 = (d - d1.astype(f32)).astype(bf16)
        d3 = (d - d1.astype(f32) - d2.astype(f32)).astype(bf16)
        out[96:112, :256] = jnp.concatenate([hi, jnp.concatenate([d1, d2], axis=1)], axis=0)
        out[96:112, 256:] = jnp.concatenate([lo, jnp.concatenate([d3, d3], axis=1)], axis=0)


def pack(at, decay, *args):
    return pl.pallas_call(
        pack_body, in_specs=[SM, SM] + [pl.BlockSpec(memory_space=pltpu.HBM)] * 7, out_specs=[VM] * 2,
        out_shape=[jax.ShapeDtypeStruct((ROWS, 512), bf16)] * 2,
        scratch_shapes=[pltpu.VMEM(a.shape, a.dtype) for a in args] + [pltpu.SemaphoreType.DMA((7,))], name="pack",
    )(at, decay, *args)


def merge_body(at, r0, r1, weights, pq_rows, rates):
    def place(a, b):
        for i, r in enumerate((a, b)):
            weights[i * 32:i * 32 + 32, :] = r[0:32, :]
            weights[64 + i * 32:96 + i * 32, :] = r[64:96, :]
            pq_rows[i * 32:i * 32 + 32, :] = r[32:64, :]
        weights[128:144, :] = jnp.concatenate([a[96:112, :].astype(f32)[:8], b[96:112, :].astype(f32)[:8]], axis=0).astype(bf16)

    @pl.when(at[1] % 2 == 0)
    def _():
        place(r0, r1)

    @pl.when(at[1] % 2 == 1)
    def _():
        place(r1, r0)

    three = r0[96:112, :].astype(f32)[8:]
    rate = (three[:, :128] + three[:, 128:256]) + three[:, 256:384]
    rates[0:8, :] = rate
    rates[8:16, :] = jnp.exp(-SPAN * rate)


def merge(at, r0, r1):
    return local(
        merge_body, in_specs=[SM] + [VM] * 2, out_specs=[VM] * 3,
        out_shape=[jax.ShapeDtypeStruct((144, 512), bf16), jax.ShapeDtypeStruct((64, 512), bf16),
                   jax.ShapeDtypeStruct((16, HALF), f32)],
        name="merge",
    )(at, r0, r1)


def join_body(a, b, c, d, out):
    for i, r in enumerate((a, b, c, d)):
        out[i * 64:i * 64 + 64, :] = r[...]


def join(parts):
    return local(join_body, in_specs=[VM] * 4, out_specs=VM, out_shape=jax.ShapeDtypeStruct((256, 512), bf16), name="join")(*parts)


def norm_body(at, tok, gain, out, full):
    z, x, c = at[0], at[2], at[3]
    v = tok[...].astype(f32)
    v = v * lax.rsqrt(jnp.mean(v * v, axis=-1, keepdims=True) + eps) * gain[...]
    full[...] = v.astype(bf16)
    lane_in = lax.broadcasted_iota(jnp.int32, (512, 512), 0)
    lane_out = lax.broadcasted_iota(jnp.int32, (512, 512), 1)
    source = (lane_out % 128) // 64 * 256 + (lane_out % 64) // 32 * 128 + (x + NX - lane_out // 128) % NX * 32 + lane_out % 32
    order = (lane_in == source).astype(bf16)
    for pair in range(NZ // 2):
        two = [full[:, pl.ds(pl.multiple_of((z + 2 * pair + i) % NZ * 512 + c * 256, 256), 256)] for i in range(2)]
        r = jnp.dot(jnp.concatenate(two, axis=1), order, preferred_element_type=f32).astype(bf16)
        for kx in range(NX):
            out[kx, :, pair * 128:pair * 128 + 128] = r[:, kx * 128:kx * 128 + 128]


def norm(at, tok, gain):
    return local(
        norm_body, in_specs=[SM, VM, VM], out_specs=VM,
        out_shape=jax.ShapeDtypeStruct((NX, HALF, 512), bf16),
        scratch_shapes=[pltpu.VMEM((HALF, 4096), bf16)], name="norm",
    )(at, tok, gain)


def split_body(at, *refs):
    z, c = at[0], at[3]
    ins, (kv, out_w, keep, give) = refs[:NZ], refs[NZ:]
    for kz in range(NZ):
        kv[kz * 64:kz * 64 + 64, :] = ins[kz][0:64, :]
        out_w[kz * 64:kz * 64 + 64, :] = ins[kz][64:128, :]
        for out, half in ((keep, c), (give, 1 - c)):
            hi = ins[kz][128:144, pl.ds(pl.multiple_of(half * HALF, HALF), HALF)].astype(f32)
            lo = ins[kz][128:144, pl.ds(pl.multiple_of(HEAD + half * HALF, HALF), HALF)].astype(f32)
            out[pl.ds(pl.multiple_of(((z + kz) % NZ) * 16, 16), 16), :] = hi + lo


def split(at, chunks):
    return local(
        split_body, in_specs=[SM] + [VM] * NZ, out_specs=[VM] * 4,
        out_shape=[jax.ShapeDtypeStruct((512, 512), bf16)] * 2 + [jax.ShapeDtypeStruct((HALF, HALF), f32)] * 2,
        name="split",
    )(at, *chunks)


def multiply(toks, pick):
    acc = None
    for kx in range(NX):
        rows = jnp.concatenate([t[kx] for t in toks], axis=0)
        r = jnp.dot(rows, pick(kx), preferred_element_type=f32)
        acc = r if acc is None else acc + r
    return acc


def span_rows(y, k):
    return pl.ds(pl.multiple_of(((y + NY - k) % NY) * HALF, HALF), HALF)


def kv_body(at, *refs):
    y, c = at[1], at[3]
    toks, ws, (kpart, vkeep, send) = refs[:4], refs[4:8], refs[8:]
    acc = multiply(toks, lambda kx: ws[kx][...])
    for k in range(NY):
        r = acc[k * HALF:(k + 1) * HALF]
        rows = span_rows(y, k)
        kpart[rows, :] = r[:, :256]
        vkeep[rows, :] = jnp.where(c == 0, r[:, 256:384], r[:, 384:])
        send[rows, :256] = r[:, :256].astype(bf16)
        send[rows, 256:] = jnp.where(c == 0, r[:, 384:], r[:, 256:384]).astype(bf16)


def project_kv(at, toks, ws):
    return local(
        kv_body, in_specs=[SM] + [VM] * 8, out_specs=[VM] * 3,
        out_shape=[jax.ShapeDtypeStruct((SPAN, HEAD), f32), jax.ShapeDtypeStruct((SPAN, HALF), f32),
                   jax.ShapeDtypeStruct((SPAN, 384), bf16)],
        name="project_kv",
    )(at, *toks, *ws)


def pq_body(at, *refs):
    toks, ws, (own, send, rhs) = refs[:4], refs[4:13], refs[13:]
    for i, kz in enumerate((0, 1, 2, 3, 5, 6, 7)):
        for kx in range(NX):
            rhs[kx, kz * 64:kz * 64 + 64, :] = ws[i][kx * 64:kx * 64 + 64, :]
    for kx in range(NX):
        rhs[kx, 256:320, :] = ws[7 + kx // 2][kx % 2 * 64:kx % 2 * 64 + 64, :]
    acc = multiply(toks, lambda kx: rhs[kx])
    for k in range(NY):
        r = acc[k * HALF:(k + 1) * HALF]
        rows = span_rows(at[1], k)
        own[rows, :] = r
        send[rows, :] = r.astype(bf16)


def project_pq(at, toks, ws):
    return local(
        pq_body, in_specs=[SM] + [VM] * 13, out_specs=[VM] * 2,
        out_shape=[jax.ShapeDtypeStruct((SPAN, 512), f32), jax.ShapeDtypeStruct((SPAN, 512), bf16)],
        scratch_shapes=[pltpu.VMEM((NX, 512, 512), bf16)], name="project_pq",
    )(at, *toks, *ws)


def turn(v, cosine, sine):
    a, b = v[:, :HALF], v[:, HALF:]
    return jnp.concatenate([a * cosine - b * sine, a * sine + b * cosine], axis=1)


def state_body(at, rates, kpart, vkeep, got, cosine, sine, keep, other, rk, val, sent, start):
    z, c = at[0], at[3]
    for zs in range(NZ):
        start[pl.ds(pl.multiple_of(zs * 32 + c * 16, 16), 16), :] = keep[zs * 16:zs * 16 + 16, :]
        start[pl.ds(pl.multiple_of(zs * 32 + (1 - c) * 16, 16), 16), :] = other[zs * 16:zs * 16 + 16, :]
    key = (kpart[...] + got[:, :256].astype(f32)).astype(bf16).astype(f32)
    value = (vkeep[...] + got[:, 256:].astype(f32)).astype(bf16)
    val[...] = value
    turned = turn(key, cosine[...], sine[...]) * HEAD ** -0.5
    rk[...] = turned.astype(bf16)
    within = lax.broadcasted_iota(jnp.int32, (SPAN, HALF), 0).astype(f32)
    fade = jnp.exp(-(SPAN - 1.0 - within) * rates[0:1, :])
    faded = (turned * jnp.concatenate([fade, fade], axis=1)).astype(bf16)
    s = lax.dot_general(faded, value, (((0,), (0,)), ((), ())), preferred_element_type=f32)
    s = s + jnp.where(z == 0, rates[8:9, :], 0.0) * start[...]
    sent[...] = s.astype(bf16)


def span_state(at, rates, *args):
    return local(
        state_body, in_specs=[SM] + [VM] * 8, out_specs=[VM] * 4,
        out_shape=[jax.ShapeDtypeStruct((SPAN, HEAD), bf16), jax.ShapeDtypeStruct((SPAN, HALF), bf16),
                   jax.ShapeDtypeStruct((HEAD, HALF), bf16), jax.ShapeDtypeStruct((HEAD, HALF), f32)],
        name="span_state",
    )(at, rates, *args)


def pool_sum_body(own, got, pool_in, tail):
    p = (own[:, :256] + got[:, :256].astype(f32)).astype(bf16)
    pool_in[...] = p
    tail[...] = p[SPAN - HALO:]


def pool_sum(own, got):
    return local(
        pool_sum_body, in_specs=[VM] * 2, out_specs=[VM] * 2,
        out_shape=[jax.ShapeDtypeStruct((SPAN, HEAD), bf16), jax.ShapeDtypeStruct((HALO, HEAD), bf16)], name="pool_sum",
    )(own, got)


def inside_body(rates, own, got, cosine, sine, rk, val, inside, faded):
    query = (own[:, 256:] + got[:, 256:].astype(f32)).astype(bf16).astype(f32)
    rq = turn(query, cosine[...], sine[...])
    within = lax.broadcasted_iota(jnp.int32, (SPAN, HALF), 0).astype(f32)
    fade = jnp.exp(-(within + 1.0) * rates[0:1, :])
    faded[...] = (rq * jnp.concatenate([fade, fade], axis=1)).astype(bf16)
    rq = rq.astype(bf16)
    for b in range(4):
        n = (b + 1) * 128
        scores = lax.dot_general(rq[b * 128:n], rk[:n, :], (((1,), (1,)), ((), ())), preferred_element_type=f32)
        far = lax.broadcasted_iota(jnp.int32, (128, n), 0) + b * 128 - lax.broadcasted_iota(jnp.int32, (128, n), 1)
        fade = jnp.exp(-jnp.maximum(far, 0).astype(f32) * jnp.concatenate([rates[0:1, :]] * (b + 1), axis=1))
        weights = jnp.where(far >= 0, scores * fade, 0.0).astype(bf16)
        inside[b * 128:n, :] = jnp.dot(weights, val[:n, :], preferred_element_type=f32)


def inside_span(rates, *args):
    return local(
        inside_body, in_specs=[VM] * 7, out_specs=[VM] * 2,
        out_shape=[jax.ShapeDtypeStruct((SPAN, HALF), f32),
                   jax.ShapeDtypeStruct((SPAN, HEAD), bf16)],
        name="inside",
    )(rates, *args)


def across_body(at, rates, inside, faded, start, *refs):
    earlier, ret = refs[:NZ - 1], refs[NZ - 1]
    d = rates[8:9, :]
    carried = earlier[NZ - 2][...].astype(f32)
    for r in reversed(earlier[:NZ - 2]):
        carried = r[...].astype(f32) + d * carried
    carried = carried + jnp.where(at[0] == 0, 1.0, 0.0) * start[...]
    ret[...] = inside[...] + jnp.dot(faded[...], carried.astype(bf16), preferred_element_type=f32)


def across_spans(at, rates, inside, faded, start, earlier):
    return local(
        across_body, in_specs=[SM] + [VM] * (NZ + 3), out_specs=VM,
        out_shape=jax.ShapeDtypeStruct((SPAN, HALF), f32), name="across",
    )(at, rates, inside, faded, start, *earlier)


def pool_body(at, pool_in, before, group_map, scale, out):
    z, y = at[0], at[1]
    ext = jnp.concatenate([before[...], pool_in[...]], axis=0).astype(f32)
    sums = ext
    chosen = None
    for g in range(4):
        sums = sums + pltpu.roll(sums, 2 ** g, 0)
        chosen = sums if chosen is None else jnp.where(y == g, sums, chosen)
    rows = lax.broadcasted_iota(jnp.int32, (SPAN, HEAD), 0) + z * SPAN + 1
    counts = jnp.minimum(lax.shift_left(jnp.int32(2), y), rows).astype(f32)
    differ = (chosen[HALO:] / counts - ext[HALO:]).astype(bf16)
    out[...] = (jnp.dot(differ, group_map[y], preferred_element_type=f32) * scale[:, pl.ds(pl.multiple_of(y * HEAD, HEAD), HEAD)]).astype(bf16)


def pooling(at, *args):
    return local(
        pool_body, in_specs=[SM] + [VM] * 4, out_specs=VM,
        out_shape=jax.ShapeDtypeStruct((SPAN, HEAD), bf16), name="pooling",
    )(at, *args)


def back_body(at, pool, ret, other, *refs):
    y, c = at[1], at[3]
    ws, outs, act, res = refs[:4], refs[4:8], refs[8], refs[9]
    r, o = ret[...], other[...]
    square = jnp.sum(r * r, axis=-1, keepdims=True) + jnp.sum(o * o, axis=-1, keepdims=True)
    factor = lax.rsqrt(square * (1.0 / HEAD) + eps)
    act[:, :256] = pool[...]
    act[:, pl.ds(pl.multiple_of(HEAD + c * HALF, HALF), HALF)] = (r * factor).astype(bf16)
    act[:, pl.ds(pl.multiple_of(HEAD + (1 - c) * HALF, HALF), HALF)] = (o * factor).astype(bf16)
    for kx in range(NX):
        r = lax.dot_general(act[...], ws[kx][...], (((1,), (1,)), ((), ())), preferred_element_type=f32)
        res[:, kx * 512:kx * 512 + 512] = r.astype(bf16)
    for k, out in enumerate(outs):
        out[...] = res[pl.ds(pl.multiple_of(((y + k) % NY) * HALF, HALF), HALF), :]


def back(at, pool, ret, other, ws):
    return local(
        back_body, in_specs=[SM] + [VM] * 7, out_specs=[VM] * 4,
        out_shape=[jax.ShapeDtypeStruct((HALF, 2048), bf16)] * 4,
        scratch_shapes=[pltpu.VMEM((SPAN, 512), bf16), pltpu.VMEM((SPAN, 2048), bf16)], name="back",
    )(at, pool, ret, other, *ws)


def total_body(at, s0, s1, s2, s3, keep, give):
    c = at[3]
    for out, half in ((keep, c), (give, 1 - c)):
        rows = pl.ds(pl.multiple_of(half * 64, 64), 64)
        out[...] = (s0[rows, :].astype(f32) + s1[rows, :].astype(f32) + (s2[rows, :].astype(f32) + s3[rows, :].astype(f32))).astype(bf16)


def total(at, arrived):
    return local(
        total_body, in_specs=[SM] + [VM] * 4, out_specs=[VM] * 2,
        out_shape=[jax.ShapeDtypeStruct((64, 2048), bf16)] * 2, name="total",
    )(at, *arrived)


def mixed_body(at, keep, got, out):
    z, x, c = at[0], at[2], at[3]
    lane_in = lax.broadcasted_iota(jnp.int32, (512, 512), 0)
    lane_out = lax.broadcasted_iota(jnp.int32, (512, 512), 1)
    source = (x + NX - (lane_out % 128) // 32) % NX * 128 + lane_out // 256 * 64 + (lane_out % 256) // 128 * 32 + lane_out % 32
    order = (lane_in == source).astype(bf16)
    for pair in range(NZ // 2):
        for ref, core in ((keep, c), (got, 1 - c)):
            rows = jnp.concatenate([ref[:, kx * 512 + pair * 128:kx * 512 + pair * 128 + 128] for kx in range(NX)], axis=1)
            r = jnp.dot(rows, order, preferred_element_type=f32).astype(bf16)
            for i in range(2):
                out[:, pl.ds(pl.multiple_of((z + 2 * pair + i) % NZ * 512 + core * 256, 256), 256)] = r[:, i * 256:i * 256 + 256]


def mixed(at, keep, got):
    return local(
        mixed_body, in_specs=[SM] + [VM] * 2, out_specs=VM,
        out_shape=jax.ShapeDtypeStruct((64, 4096), bf16), name="mixed",
    )(at, keep, got)


def layer(tokens, norm_gain, pool_proj, query_proj, key_proj, value_proj, pool_map, pool_scale,
          decay_rate, start_state, pool_back, retention_back):
    z, y, x, c = (lax.axis_index(a) for a in ("z", "y", "x", "c"))
    at = jnp.stack([z, y, x, c]).astype(jnp.int32)

    s0, s1 = pack(at, decay_rate, pool_proj, query_proj, key_proj, value_proj, start_state[0], pool_back.T, retention_back.T)
    r0 = lax.ppermute(s0, ("y", "c"), to_heads(0))
    r1 = lax.ppermute(s1, ("y", "c"), to_heads(1))
    shard_in, shard_pq, rates = merge(at, r0, r1)

    toks = [norm(at, tokens[0], norm_gain[None])]
    for k in (1, 2, 3):
        toks.append(lax.ppermute(toks[0], "y", ring(NY, k)))


    in_z = z_ring(shard_in, False)
    plane_kv, plane_out, keep, give = split(at, in_z)
    kv_list = direct(plane_kv, "x", NX)
    out_list = direct(plane_out, "x", NX)
    start_other = swap(give)

    plane_pq = join(direct(shard_pq, "x", NX))
    pq_list = z_ring(plane_pq, True)

    positions = (jnp.arange(SPAN, dtype=jnp.int32) + z * SPAN)
    inv_freq = 1.0 / rope_base ** jnp.linspace(0.0, 1.0, HALF, dtype=f32)
    angles = positions.astype(f32)[:, None] * inv_freq[None, :]
    cosine, sine = jnp.cos(angles), jnp.sin(angles)

    kpart, vkeep, send = project_kv(at, toks, kv_list)
    got = swap(send)
    rk, val, sent, start = span_state(at, rates, kpart, vkeep, got, cosine, sine, keep, start_other)
    earlier = [lax.ppermute(sent, "z", line(NZ, k)) for k in range(1, NZ)]

    own, send = project_pq(at, toks, pq_list)
    got = swap(send)
    pool_in, tail = pool_sum(own, got)
    inside, faded = inside_span(rates, own, got, cosine, sine, rk, val)
    before = lax.ppermute(tail, "z", line(NZ, 1))
    pool_out = pooling(at, pool_in, before, pool_map, pool_scale[None])
    ret = across_spans(at, rates, inside, faded, start, earlier)
    other = swap(ret)

    shares = back(at, pool_out, ret, other, out_list)
    arrived = [shares[0]] + [lax.ppermute(shares[k], "y", ring(NY, k)) for k in range(1, NY)]
    keep, give = total(at, arrived)
    got = swap(give)
    return mixed(at, keep, got)[None]


def solution(mesh):
    torus = Mesh(mesh.devices.reshape(NZ, NY, NX, 2), ("z", "y", "x", "c"))
    sp, sp_fs = ("z", "y"), ("z", "y", "x")
    placed = (
        P("x", sp, None), P(), P(sp_fs, "c"), P(sp_fs, "c"), P(sp_fs, "c"), P(sp_fs, "c"), P(), P(),
        P("c"), P("x", "c", sp, None), P("c", sp_fs), P("c", sp_fs),
    )
    return jax.shard_map(layer, mesh=torus, in_specs=placed, out_specs=P("x", ("z", "y", "c"), None), check_vma=False)
```

```python
import jax
import jax.numpy as jnp
from jax import lax
from jax.experimental import pallas as pl
from jax.experimental.pallas import tpu as pltpu
from jax.sharding import Mesh
from jax.sharding import PartitionSpec as P

NZ, NY, NX = 8, 4, 4
SPAN = 512
ORDER = (0, 1, 7, 2, 6, 3, 5, 4)
EARLY = 6
HALO = 16
HEAD = 256
HALF = 128
eps = 1e-06
rope_base = 10000.0

bf16 = jnp.bfloat16
f32 = jnp.float32


def ring(n, k):
    return [(i, (i + k) % n) for i in range(n)]


def line(n, k):
    return [(i, i + k) for i in range(n - k)]


def to_heads(k):
    return [(2 * y + c, 2 * (2 * c + (k + y) % 2) + y // 2) for y in range(NY) for c in range(2)]


SWAP = [(0, 1), (1, 0)]


def swap(a):
    return lax.ppermute(a, "c", SWAP)


def direct(a, axis, n):
    return [a] + [lax.ppermute(a, axis, ring(n, k)) for k in range(1, n)]


def z_ring(a, halves):
    chunks = [None] * NZ
    chunks[0] = a
    up = down = a
    for s in range(1, 4):
        up = lax.ppermute(up, "z", ring(NZ, 1))
        down = lax.ppermute(down, "z", ring(NZ, -1))
        chunks[NZ - s], chunks[s] = up, down
    if not halves:
        chunks[4] = lax.ppermute(up, "z", ring(NZ, 1))
        return chunks
    n = a.shape[0] // 2
    return chunks[:4] + chunks[5:] + [lax.ppermute(up[:n], "z", ring(NZ, 1)), lax.ppermute(down[n:], "z", ring(NZ, -1))]


VM = pl.BlockSpec(memory_space=pltpu.VMEM)
SM = pl.BlockSpec(memory_space=pltpu.SMEM)
ANY = pl.BlockSpec(memory_space=pl.ANY)


def local(body, **kw):
    return pl.pallas_call(body, compiler_params=pltpu.CompilerParams(vmem_limit_bytes=16 * 2**20), **kw)


ROWS = 112


def pack_body(at, decay, *refs):
    y = at[1]
    sources, (s0, s1), held, sem = refs[:7], refs[7:9], refs[9:16], refs[16]
    copies = [pltpu.make_async_copy(a, b, sem.at[i]) for i, (a, b) in enumerate(zip(sources, held))]
    for cp in copies:
        cp.start()
    for cp in copies:
        cp.wait()
    pool, query, key, value, state, pback, rback = held
    for k, out in enumerate((s0, s1)):
        p = (y + k) % 2
        at_head = pl.ds(pl.multiple_of(p * HEAD, HEAD), HEAD)
        out[0:32, :256] = key[:, at_head]
        out[0:32, 256:] = value[:, at_head]
        out[32:64, :256] = pool[:, at_head]
        out[32:64, 256:] = query[:, at_head]
        out[64:96, :256] = pback[:, at_head]
        out[64:96, 256:] = rback[:, at_head]
        s = state[p]
        hi = s.astype(bf16)
        lo = (s - hi.astype(f32)).astype(bf16)
        d = jnp.full((8, HALF), decay[p], f32)
        d1 = d.astype(bf16)
        d2 = (d - d1.astype(f32)).astype(bf16)
        d3 = (d - d1.astype(f32) - d2.astype(f32)).astype(bf16)
        out[96:112, :256] = jnp.concatenate([hi, jnp.concatenate([d1, d2], axis=1)], axis=0)
        out[96:112, 256:] = jnp.concatenate([lo, jnp.concatenate([d3, d3], axis=1)], axis=0)


def pack(at, decay, *args):
    return pl.pallas_call(
        pack_body, in_specs=[SM, SM] + [pl.BlockSpec(memory_space=pltpu.HBM)] * 7, out_specs=[VM] * 2,
        out_shape=[jax.ShapeDtypeStruct((ROWS, 512), bf16)] * 2,
        scratch_shapes=[pltpu.VMEM(a.shape, a.dtype) for a in args] + [pltpu.SemaphoreType.DMA((7,))], name="pack",
    )(at, decay, *args)


def merge_body(at, r0, r1, weights, pq_rows, rates):
    def place(a, b):
        for i, r in enumerate((a, b)):
            weights[i * 32:i * 32 + 32, :] = r[0:32, :]
            weights[64 + i * 32:96 + i * 32, :] = r[64:96, :]
            pq_rows[i * 32:i * 32 + 32, :] = r[32:64, :]
        weights[128:144, :] = jnp.concatenate([a[96:112, :].astype(f32)[:8], b[96:112, :].astype(f32)[:8]], axis=0).astype(bf16)

    @pl.when(at[1] % 2 == 0)
    def _():
        place(r0, r1)

    @pl.when(at[1] % 2 == 1)
    def _():
        place(r1, r0)

    three = r0[96:112, :].astype(f32)[8:]
    rate = (three[:, :128] + three[:, 128:256]) + three[:, 256:384]
    rates[0:8, :] = rate
    rates[8:16, :] = jnp.exp(-SPAN * rate)


def merge(at, r0, r1):
    return local(
        merge_body, in_specs=[SM] + [VM] * 2, out_specs=[VM] * 3,
        out_shape=[jax.ShapeDtypeStruct((144, 512), bf16), jax.ShapeDtypeStruct((64, 512), bf16),
                   jax.ShapeDtypeStruct((16, HALF), f32)],
        name="merge",
    )(at, r0, r1)


def join_body(a, b, c, d, out):
    for i, r in enumerate((a, b, c, d)):
        out[i * 64:i * 64 + 64, :] = r[...]


def join(parts):
    return local(join_body, in_specs=[VM] * 4, out_specs=VM, out_shape=jax.ShapeDtypeStruct((256, 512), bf16), name="join")(*parts)


def norm_body(at, tok, gain, out, full):
    z, x, c = at[0], at[2], at[3]

    @pl.loop(0, HALF // 16)
    def _(i):
        rows = pl.ds(pl.multiple_of(i * 16, 16), 16)
        v = tok[rows, :].astype(f32)
        v = v * lax.rsqrt(jnp.mean(v * v, axis=-1, keepdims=True) + eps) * gain[...]
        full[rows, :] = v.astype(bf16)

    lane_in = lax.broadcasted_iota(jnp.int32, (512, 512), 0)
    lane_out = lax.broadcasted_iota(jnp.int32, (512, 512), 1)
    source = (lane_out % 128) // 64 * 256 + (lane_out % 64) // 32 * 128 + (x + NX - lane_out // 128) % NX * 32 + lane_out % 32
    order = (lane_in == source).astype(bf16)
    for pair in range(NZ // 2):
        two = [full[:, pl.ds(pl.multiple_of((z + ORDER[2 * pair + i]) % NZ * 512 + c * 256, 256), 256)] for i in range(2)]
        r = jnp.dot(jnp.concatenate(two, axis=1), order, preferred_element_type=f32).astype(bf16)
        for kx in range(NX):
            out[kx, :, pair * 128:pair * 128 + 128] = r[:, kx * 128:kx * 128 + 128]


def norm(at, tok, gain):
    return local(
        norm_body, in_specs=[SM, VM, VM], out_specs=VM,
        out_shape=jax.ShapeDtypeStruct((NX, HALF, 512), bf16),
        scratch_shapes=[pltpu.VMEM((HALF, 4096), bf16)], name="norm",
    )(at, tok, gain)


def early_body(*refs):
    for i in range(EARLY):
        refs[EARLY][i * 64:i * 64 + 64, :] = refs[i][0:64, :]


def split_early(chunks):
    return local(
        early_body, in_specs=[VM] * EARLY, out_specs=VM,
        out_shape=jax.ShapeDtypeStruct((EARLY * 64, 512), bf16), name="split_early",
    )(*[chunks[kz] for kz in ORDER[:EARLY]])


def late_body(at, *refs):
    z, c = at[0], at[3]
    ins, (kv, out_w, keep, give) = refs[:NZ], refs[NZ:]
    for i, kz in enumerate(ORDER[EARLY:]):
        kv[i * 64:i * 64 + 64, :] = ins[kz][0:64, :]
    for kz in range(NZ):
        out_w[kz * 64:kz * 64 + 64, :] = ins[kz][64:128, :]
        for out, half in ((keep, c), (give, 1 - c)):
            hi = ins[kz][128:144, pl.ds(pl.multiple_of(half * HALF, HALF), HALF)].astype(f32)
            lo = ins[kz][128:144, pl.ds(pl.multiple_of(HEAD + half * HALF, HALF), HALF)].astype(f32)
            out[pl.ds(pl.multiple_of(((z + kz) % NZ) * 16, 16), 16), :] = hi + lo


def split_late(at, chunks):
    return local(
        late_body, in_specs=[SM] + [VM] * NZ, out_specs=[VM] * 4,
        out_shape=[jax.ShapeDtypeStruct(((NZ - EARLY) * 64, 512), bf16), jax.ShapeDtypeStruct((512, 512), bf16)]
        + [jax.ShapeDtypeStruct((HALF, HALF), f32)] * 2,
        name="split_late",
    )(at, *chunks)


def multiply(toks, pick):
    acc = None
    for kx in range(NX):
        rows = jnp.concatenate([t[kx] for t in toks], axis=0)
        r = jnp.dot(rows, pick(kx), preferred_element_type=f32)
        acc = r if acc is None else acc + r
    return acc


def span_rows(y, k):
    return pl.ds(pl.multiple_of(((y + NY - k) % NY) * HALF, HALF), HALF)


def kv_body(at, *refs):
    y, c = at[1], at[3]
    toks, early, late, (kpart, vkeep, send) = refs[:4], refs[4:8], refs[8:12], refs[12:]
    acc = multiply(toks, lambda kx: jnp.concatenate([early[kx][...], late[kx][...]], axis=0))
    for k in range(NY):
        r = acc[k * HALF:(k + 1) * HALF]
        rows = span_rows(y, k)
        kpart[rows, :] = r[:, :256]
        vkeep[rows, :] = jnp.where(c == 0, r[:, 256:384], r[:, 384:])
        send[rows, :256] = r[:, :256].astype(bf16)
        send[rows, 256:] = jnp.where(c == 0, r[:, 384:], r[:, 256:384]).astype(bf16)


def project_kv(at, toks, ws):
    return local(
        kv_body, in_specs=[SM] + [VM] * 12, out_specs=[VM] * 3,
        out_shape=[jax.ShapeDtypeStruct((SPAN, HEAD), f32), jax.ShapeDtypeStruct((SPAN, HALF), f32),
                   jax.ShapeDtypeStruct((SPAN, 384), bf16)],
        name="project_kv",
    )(at, *toks, *ws)


def pq_body(at, *refs):
    toks, ws, (own, send, rhs) = refs[:4], refs[4:12], refs[12:]
    for kz in range(NZ):
        for kx in range(NX):
            rhs[kx, ORDER.index(kz) * 64:ORDER.index(kz) * 64 + 64, :] = ws[kz][kx * 64:kx * 64 + 64, :]
    acc = multiply(toks, lambda kx: rhs[kx])
    for k in range(NY):
        r = acc[k * HALF:(k + 1) * HALF]
        rows = span_rows(at[1], k)
        own[rows, :] = r
        send[rows, :] = r.astype(bf16)


def project_pq(at, toks, ws):
    return local(
        pq_body, in_specs=[SM] + [VM] * 12, out_specs=[VM] * 2,
        out_shape=[jax.ShapeDtypeStruct((SPAN, 512), f32), jax.ShapeDtypeStruct((SPAN, 512), bf16)],
        scratch_shapes=[pltpu.VMEM((NX, 512, 512), bf16)], name="project_pq",
    )(at, *toks, *ws)


def turn(v, cosine, sine):
    a, b = v[:, :HALF], v[:, HALF:]
    return jnp.concatenate([a * cosine - b * sine, a * sine + b * cosine], axis=1)


def state_body(at, rates, kpart, vkeep, got, cosine, sine, keep, other, rk, val, sent, start):
    z, c = at[0], at[3]
    for zs in range(NZ):
        start[pl.ds(pl.multiple_of(zs * 32 + c * 16, 16), 16), :] = keep[zs * 16:zs * 16 + 16, :]
        start[pl.ds(pl.multiple_of(zs * 32 + (1 - c) * 16, 16), 16), :] = other[zs * 16:zs * 16 + 16, :]
    key = (kpart[...] + got[:, :256].astype(f32)).astype(bf16).astype(f32)
    value = (vkeep[...] + got[:, 256:].astype(f32)).astype(bf16)
    val[...] = value
    turned = turn(key, cosine[...], sine[...]) * HEAD ** -0.5
    rk[...] = turned.astype(bf16)
    within = lax.broadcasted_iota(jnp.int32, (SPAN, HALF), 0).astype(f32)
    fade = jnp.exp(-(SPAN - 1.0 - within) * rates[0:1, :])
    faded = (turned * jnp.concatenate([fade, fade], axis=1)).astype(bf16)
    s = lax.dot_general(faded, value, (((0,), (0,)), ((), ())), preferred_element_type=f32)
    s = s + jnp.where(z == 0, rates[8:9, :], 0.0) * start[...]
    sent[...] = s.astype(bf16)


def span_state(at, rates, *args):
    return local(
        state_body, in_specs=[SM] + [VM] * 8, out_specs=[VM] * 4,
        out_shape=[jax.ShapeDtypeStruct((SPAN, HEAD), bf16), jax.ShapeDtypeStruct((SPAN, HALF), bf16),
                   jax.ShapeDtypeStruct((HEAD, HALF), bf16), jax.ShapeDtypeStruct((HEAD, HALF), f32)],
        name="span_state",
    )(at, rates, *args)


def pool_sum_body(own, got, pool_in, tail):
    p = (own[:, :256] + got[:, :256].astype(f32)).astype(bf16)
    pool_in[...] = p
    tail[...] = p[SPAN - HALO:]


def pool_sum(own, got):
    return local(
        pool_sum_body, in_specs=[VM] * 2, out_specs=[VM] * 2,
        out_shape=[jax.ShapeDtypeStruct((SPAN, HEAD), bf16), jax.ShapeDtypeStruct((HALO, HEAD), bf16)], name="pool_sum",
    )(own, got)


def inside_body(rates, own, got, cosine, sine, rk, val, inside, faded):
    query = (own[:, 256:] + got[:, 256:].astype(f32)).astype(bf16).astype(f32)
    rq = turn(query, cosine[...], sine[...])
    within = lax.broadcasted_iota(jnp.int32, (SPAN, HALF), 0).astype(f32)
    fade = jnp.exp(-(within + 1.0) * rates[0:1, :])
    faded[...] = (rq * jnp.concatenate([fade, fade], axis=1)).astype(bf16)
    rq = rq.astype(bf16)
    for b in range(4):
        n = (b + 1) * 128
        scores = lax.dot_general(rq[b * 128:n], rk[:n, :], (((1,), (1,)), ((), ())), preferred_element_type=f32)
        far = lax.broadcasted_iota(jnp.int32, (128, n), 0) + b * 128 - lax.broadcasted_iota(jnp.int32, (128, n), 1)
        fade = jnp.exp(-jnp.maximum(far, 0).astype(f32) * jnp.concatenate([rates[0:1, :]] * (b + 1), axis=1))
        weights = jnp.where(far >= 0, scores * fade, 0.0).astype(bf16)
        inside[b * 128:n, :] = jnp.dot(weights, val[:n, :], preferred_element_type=f32)


def inside_span(rates, *args):
    return local(
        inside_body, in_specs=[VM] * 7, out_specs=[VM] * 2,
        out_shape=[jax.ShapeDtypeStruct((SPAN, HALF), f32),
                   jax.ShapeDtypeStruct((SPAN, HEAD), bf16)],
        name="inside",
    )(rates, *args)


def across_body(at, rates, inside, faded, start, *refs):
    earlier, ret = refs[:NZ - 1], refs[NZ - 1]
    d = rates[8:9, :]
    carried = earlier[NZ - 2][...].astype(f32)
    for r in reversed(earlier[:NZ - 2]):
        carried = r[...].astype(f32) + d * carried
    carried = carried + jnp.where(at[0] == 0, 1.0, 0.0) * start[...]
    ret[...] = inside[...] + jnp.dot(faded[...], carried.astype(bf16), preferred_element_type=f32)


def across_spans(at, rates, inside, faded, start, earlier):
    return local(
        across_body, in_specs=[SM] + [VM] * (NZ + 3), out_specs=VM,
        out_shape=jax.ShapeDtypeStruct((SPAN, HALF), f32), name="across",
    )(at, rates, inside, faded, start, *earlier)


def pool_body(at, pool_in, before, group_map, scale, out):
    z, y = at[0], at[1]
    ext = jnp.concatenate([before[...], pool_in[...]], axis=0).astype(f32)
    sums = ext
    chosen = None
    for g in range(4):
        sums = sums + pltpu.roll(sums, 2 ** g, 0)
        chosen = sums if chosen is None else jnp.where(y == g, sums, chosen)
    rows = lax.broadcasted_iota(jnp.int32, (SPAN, HEAD), 0) + z * SPAN + 1
    counts = jnp.minimum(lax.shift_left(jnp.int32(2), y), rows).astype(f32)
    differ = (chosen[HALO:] / counts - ext[HALO:]).astype(bf16)
    out[...] = (jnp.dot(differ, group_map[y], preferred_element_type=f32) * scale[:, pl.ds(pl.multiple_of(y * HEAD, HEAD), HEAD)]).astype(bf16)


def pooling(at, *args):
    return local(
        pool_body, in_specs=[SM] + [VM] * 4, out_specs=VM,
        out_shape=jax.ShapeDtypeStruct((SPAN, HEAD), bf16), name="pooling",
    )(at, *args)


def back_body(at, pool, ret, other, *refs):
    y, c = at[1], at[3]
    ws, outs, act, res = refs[:4], refs[4:12], refs[12], refs[13]
    r, o = ret[...], other[...]
    square = jnp.sum(r * r, axis=-1, keepdims=True) + jnp.sum(o * o, axis=-1, keepdims=True)
    factor = lax.rsqrt(square * (1.0 / HEAD) + eps)
    act[:, :256] = pool[...]
    act[:, pl.ds(pl.multiple_of(HEAD + c * HALF, HALF), HALF)] = (r * factor).astype(bf16)
    act[:, pl.ds(pl.multiple_of(HEAD + (1 - c) * HALF, HALF), HALF)] = (o * factor).astype(bf16)
    for kx in range(NX):
        r = lax.dot_general(act[...], ws[kx][...], (((1,), (1,)), ((), ())), preferred_element_type=f32)
        res[:, kx * 512:kx * 512 + 512] = r.astype(bf16)
    for k in range(NY):
        for cross, half in enumerate((c, 1 - c)):
            first = ((y + k) % NY) * HALF + half * 64
            outs[2 * k + cross][...] = res[pl.ds(pl.multiple_of(first, 64), 64), :]


def back(at, pool, ret, other, ws):
    return local(
        back_body, in_specs=[SM] + [VM] * 7, out_specs=[VM] * 8,
        out_shape=[jax.ShapeDtypeStruct((64, 2048), bf16)] * 8,
        scratch_shapes=[pltpu.VMEM((SPAN, 512), bf16), pltpu.VMEM((SPAN, 2048), bf16)], name="back",
    )(at, pool, ret, other, *ws)


def owner(k, cross):
    return [(2 * y + c, 2 * ((y + k) % NY) + (c ^ cross)) for y in range(NY) for c in range(2)]


def mixed_body(at, *refs):
    z, x, c = at[0], at[2], at[3]
    shares, out, total = refs[:8], refs[8], refs[9]
    lane_in = lax.broadcasted_iota(jnp.int32, (512, 512), 0)
    lane_out = lax.broadcasted_iota(jnp.int32, (512, 512), 1)
    source = (x + NX - (lane_out % 128) // 32) % NX * 128 + lane_out // 256 * 64 + (lane_out % 256) // 128 * 32 + lane_out % 32
    order = (lane_in == source).astype(bf16)
    for cross in range(2):
        a, b, d, e = (shares[2 * k + cross][...].astype(f32) for k in range(NY))
        total[cross * 64:cross * 64 + 64, :] = ((a + b) + (d + e)).astype(bf16)

    @pl.loop(0, NZ // 2)
    def _(pair):
        at_pair = [pl.ds(pl.multiple_of(kx * 512 + pair * 128, 128), 128) for kx in range(NX)]
        rows = jnp.concatenate([total[:, lanes] for lanes in at_pair], axis=1)
        r = jnp.dot(rows, order, preferred_element_type=f32).astype(bf16)
        for cross, core in enumerate((c, 1 - c)):
            for i in range(2):
                lanes = pl.ds(pl.multiple_of((z + 2 * pair + i) % NZ * 512 + core * 256, 256), 256)
                out[:, lanes] = r[cross * 64:cross * 64 + 64, i * 256:i * 256 + 256]


def mixed(at, shares):
    return local(
        mixed_body, in_specs=[SM] + [VM] * 8, out_specs=VM,
        out_shape=jax.ShapeDtypeStruct((64, 4096), bf16),
        scratch_shapes=[pltpu.VMEM((2 * 64, 2048), bf16)], name="mixed",
    )(at, *shares)


def layer(tokens, norm_gain, pool_proj, query_proj, key_proj, value_proj, pool_map, pool_scale,
          decay_rate, start_state, pool_back, retention_back):
    z, y, x, c = (lax.axis_index(a) for a in ("z", "y", "x", "c"))
    at = jnp.stack([z, y, x, c]).astype(jnp.int32)

    s0, s1 = pack(at, decay_rate, pool_proj, query_proj, key_proj, value_proj, start_state[0], pool_back.T, retention_back.T)
    r0 = lax.ppermute(s0, ("y", "c"), to_heads(0))
    r1 = lax.ppermute(s1, ("y", "c"), to_heads(1))
    shard_in, shard_pq, rates = merge(at, r0, r1)

    toks = [norm(at, tokens[0], norm_gain[None])]
    for k in (1, 2, 3):
        toks.append(lax.ppermute(toks[0], "y", ring(NY, k)))


    in_z = z_ring(shard_in, False)
    kv_list = direct(split_early(in_z), "x", NX)
    plane_kv, plane_out, keep, give = split_late(at, in_z)
    kv_list = kv_list + direct(plane_kv, "x", NX)
    out_list = direct(plane_out, "x", NX)
    start_other = swap(give)

    plane_pq = join(direct(shard_pq, "x", NX))
    pq_list = z_ring(plane_pq, False)

    positions = (jnp.arange(SPAN, dtype=jnp.int32) + z * SPAN)
    inv_freq = 1.0 / rope_base ** jnp.linspace(0.0, 1.0, HALF, dtype=f32)
    angles = positions.astype(f32)[:, None] * inv_freq[None, :]
    cosine, sine = jnp.cos(angles), jnp.sin(angles)

    kpart, vkeep, send = project_kv(at, toks, kv_list)
    got = swap(send)
    rk, val, sent, start = span_state(at, rates, kpart, vkeep, got, cosine, sine, keep, start_other)
    earlier = [lax.ppermute(sent, "z", line(NZ, k)) for k in range(1, NZ)]

    own, send = project_pq(at, toks, pq_list)
    got = swap(send)
    pool_in, tail = pool_sum(own, got)
    inside, faded = inside_span(rates, own, got, cosine, sine, rk, val)
    before = lax.ppermute(tail, "z", line(NZ, 1))
    pool_out = pooling(at, pool_in, before, pool_map, pool_scale[None])
    ret = across_spans(at, rates, inside, faded, start, earlier)
    other = swap(ret)

    shares = back(at, pool_out, ret, other, out_list)
    arrived = [shares[0]]
    for k in range(NY):
        for cross in range(2):
            if k + cross > 0:
                arrived.append(lax.ppermute(shares[2 * k + cross], ("y", "c"), owner(k, cross)))
    return mixed(at, arrived)[None]


def solution(mesh):
    torus = Mesh(mesh.devices.reshape(NZ, NY, NX, 2), ("z", "y", "x", "c"))
    sp, sp_fs = ("z", "y"), ("z", "y", "x")
    placed = (
        P("x", sp, None), P(), P(sp_fs, "c"), P(sp_fs, "c"), P(sp_fs, "c"), P(sp_fs, "c"), P(), P(),
        P("c"), P("x", "c", sp, None), P("c", sp_fs), P("c", sp_fs),
    )
    return jax.shard_map(layer, mesh=torus, in_specs=placed, out_specs=P("x", ("z", "y", "c"), None), check_vma=False)
```
